512 devices in a mesh: sp: 32 (over z, core), tp: 16 (over y, x).
Axes of the slice: x: 4, y: 4, z: 16, core: 2. Of those that a mesh axis runs over, the one named last changes fastest.
Arguments:
- query_rows: bfloat16 [8192, 2048], P('sp', 'tp'), may hold values from -1000 to 1000
- key_rows: bfloat16 [8192, 256], P('sp'), may hold values from -6 to 6
- value_rows: bfloat16 [8192, 256], P('sp'), may hold values from -6 to 6
- sink_logits: float32 [32], P('tp'), may hold values from 1 to 6
- out_weight: bfloat16 [2048, 2048], P('tp'), may hold values from -0.375 to 0.375
- stream_in: bfloat16 [8192, 2048], P('sp'), may hold values from -6 to 6
- norm_gain: float32 [2048], replicated, may hold values from 0.1 to 1.9
- routes: int32 [8192, 2], P('sp'), may hold values from 0 to 31, all different within a row; in each aligned block of 256 rows (0 to 255, 256 to 511, ...) at most 24 rows name the same one
- route_weights: float32 [8192, 2], P('sp'), may hold values from 0.2 to 1
- gate_weight: bfloat16 [32, 2048, 4096], P('sp', None, 'tp'), may hold values from -0.125 to 0.125
- up_weight: bfloat16 [32, 2048, 4096], P('sp', None, 'tp'), may hold values from -0.125 to 0.125
- down_weight: bfloat16 [32, 4096, 2048], P('sp', 'tp'), may hold values from -0.09375 to 0.09375
Outputs:
- layer_out: bfloat16 [8192, 2048], P(('sp', 'tp'))
The draws below stay inside these ranges and needn't reach their ends.
Inputs may be any that keep to these rules, and one draw needn't show every extreme that they name: `routes`: each row names 2 different experts. Within the rows of one device (256 aligned rows) no expert is named more than 24 times, a bound that some block reaches.
All inputs are finite; a program needn't handle non-finite values.
Results may differ from the reference program's by a relative error of at most 0.015.
Values may be sent and summed in bfloat16 or wider, within the bound.
No kernel may reach another device: no remote copies, remote signals or barrier semaphores. Data moves between devices by JAX's collectives and lax.ppermute only.
A program may use at most 64 MiB of HBM per device.

```python
import math
import jax
import jax.numpy as jnp
import numpy as np
from jax import lax

D = 2048
HEAD_DIM = 64
HEADS = 32
KV_HEADS = 4
REP = 8
WINDOW = 128
EXPERT_FF = 4096
TOPK = 2
TOK_SP = 256
TOKENS = 8192
EXPERTS = 32
CAP = 24
N_SP = 32
N_TP = 16


def drawn_pair(key):
    key_draw = jnp.clip(jax.random.normal(jax.random.fold_in(key, 11), (TOKENS, KV_HEADS, HEAD_DIM), jnp.float32), -6.0, 6.0)
    queries = jnp.clip(jax.random.normal(jax.random.fold_in(key, 12), (TOKENS, KV_HEADS, REP, HEAD_DIM), jnp.float32), -6.0, 6.0)
    return (key_draw, queries)


def draw_query_rows(key, part):
    key_draw, queries = drawn_pair(key)
    return queries.reshape(TOKENS, HEADS * HEAD_DIM).astype(jnp.bfloat16)


def draw_key_rows(key, part):
    key_draw, queries = drawn_pair(key)
    return key_draw.reshape(TOKENS, KV_HEADS * HEAD_DIM).astype(jnp.bfloat16)


def block_levels(rng, shape, cuts, smallest, top_value):
    level = 1.0
    for axis_at, parts in cuts:
        heights = jax.random.uniform(jax.random.fold_in(jax.random.fold_in(rng, 6), axis_at), (parts,), jnp.float32, smallest / len(cuts), top_value / len(cuts))
        level = level * jnp.repeat(jnp.exp(heights), shape[axis_at] // parts).reshape((-1,) + (1,) * (len(shape) - 1 - axis_at))
    return level


def assign_block(stream_key, own, number, rows, amount, top, limit, skew):
    order = jax.random.permutation(stream_key, amount)
    heavy_load, common = load_shares(amount, rows * top, limit, skew, True), load_shares(amount, rows * top, limit, skew, False)
    places = jnp.arange(amount)

    def named(sizes, rotation):
        used = int((sizes > 0).sum())
        fixed = max(1, used // 4)
        shifted = fixed + (places - fixed + rotation * (used - fixed)) % max(1, amount - fixed)
        return jnp.zeros((amount,), jnp.int32).at[order[jnp.where(places < fixed, places, shifted)]].set(jnp.asarray(sizes, jnp.int32))

    sizes = jnp.where(number % 4 == 0, named(heavy_load, number // 4), named(common, number - number // 4 - 1))
    mixed = jax.random.permutation(jax.random.fold_in(own, 3), amount)
    giver, sink = mixed[0:amount // 2 * 2:2], mixed[1:amount // 2 * 2:2]
    room = jnp.minimum(sizes[giver] - 1, limit - sizes[sink]) // 2
    room = jnp.where((giver == order[0]) | (sink == order[0]) | (sizes[sink] == 0), 0, jnp.maximum(room, 0))
    shifted = jax.random.randint(jax.random.fold_in(own, 4), (amount // 2,), 0, 1 << 20) % (room + 1)
    sizes = sizes.at[giver].add(-shifted).at[sink].add(shifted)
    members = jnp.searchsorted(jnp.cumsum(sizes), jnp.arange(rows * top), side="right").astype(jnp.int32)
    listing = members.reshape(top, rows).T
    listing = listing[jax.random.permutation(jax.random.fold_in(own, 1), rows)]
    rotation = jax.random.randint(jax.random.fold_in(own, 2), (rows, 1), 0, top)
    return jnp.take_along_axis(listing, (jnp.arange(top)[None, :] + rotation) % top, axis=1)


def load_shares(count, total, bound, skew, full):
    portions = [(1 << 20) // math.isqrt(grade ** skew) + 1 for grade in range(1, count + 1)]
    largest = bound if full else min(bound, max(-(-total // count), total * portions[0] // sum(portions)))
    least = 1 if total - largest >= count - 1 else 0
    given, rest = [largest] + [least] * (count - 1), total - largest - least * (count - 1)
    while rest > 0:
        candidates = [i for i in range(1, count) if given[i] < largest] or [i for i in range(1, count) if given[i] < bound]
        whole, budget = sum([portions[i] for i in candidates]), rest
        for i in candidates:
            extra = min(bound - given[i], max(1, budget * portions[i] // whole), rest)
            given[i] = given[i] + extra
            rest = rest - extra
    return np.array(given)


def scatter_about(own_key, shape, scale, bound, pieces=(), held_as=jnp.bfloat16):
    factor_of = block_levels(own_key, shape, pieces, -0.22, 0.18) if pieces else 1.0
    result = jax.random.normal(own_key, shape, jnp.float32) * scale * factor_of
    return jnp.minimum(jnp.maximum(result, -bound), bound).astype(held_as)


def setup_inputs(seed: int = 0) -> dict:
    keys = jax.random.split(jax.random.key(seed), 13)
    query_rows = draw_query_rows(jax.random.fold_in(keys[12], 71), 0)
    key_rows = draw_key_rows(jax.random.fold_in(keys[12], 71), 0)
    value_rows = scatter_about(keys[2], (TOKENS, KV_HEADS * HEAD_DIM), 1.0, 6.0, ((0, 32),))
    sink_logits = jnp.clip(1.0 + 5.0 * jax.random.uniform(keys[3], (HEADS,), jnp.float32) ** block_levels(keys[3], (HEADS,), ((0, 16),), -0.2, 0.2), 1.0, 6.0)
    out_weight = scatter_about(keys[4], (HEADS * HEAD_DIM, D), (HEADS * HEAD_DIM // 8) ** -0.5, 0.375, ((0, 16),))
    stream_in = scatter_about(keys[5], (TOKENS, D), 1.0, 6.0, ((0, 32),))
    norm_gain = jnp.clip(1.0 + 0.18 * jax.random.normal(keys[6], (D,), jnp.float32), 0.1, 1.9)
    routes_keys = jax.random.split(jax.random.fold_in(keys[7], 1), TOKENS // TOK_SP)
    routes_turns = jax.random.permutation(jax.random.fold_in(keys[7], 3), TOKENS // TOK_SP)
    routes = jax.vmap(lambda own, number: assign_block(jax.random.fold_in(keys[7], 2), own, number, TOK_SP, EXPERTS, TOPK, CAP, 1))(routes_keys, routes_turns).reshape((TOKENS, TOPK))
    route_weights = jnp.clip(0.2 + 0.8 * jax.random.uniform(keys[8], (TOKENS, TOPK), jnp.float32) ** block_levels(keys[8], (TOKENS, TOPK), ((0, 32),), -0.2, 0.2), 0.2, 1.0)
    gate_weight = scatter_about(keys[9], (EXPERTS, D, EXPERT_FF), D ** -0.5, 0.125, ((0, 32), (2, 16)))
    up_weight = scatter_about(keys[10], (EXPERTS, D, EXPERT_FF), D ** -0.5, 0.125, ((0, 32), (2, 16)))
    down_weight = scatter_about(keys[11], (EXPERTS, EXPERT_FF, D), EXPERT_FF ** -0.5, 0.09375, ((0, 32), (1, 16)))
    return dict(query_rows=query_rows, key_rows=key_rows, value_rows=value_rows, sink_logits=sink_logits, out_weight=out_weight, stream_in=stream_in, norm_gain=norm_gain, routes=routes, route_weights=route_weights, gate_weight=gate_weight, up_weight=up_weight, down_weight=down_weight)


norm_eps = 1e-06

def route_targets(block_routes):
    flat_ids = block_routes.reshape(-1)
    onehot = (flat_ids[:, None] == jnp.arange(EXPERTS, dtype=jnp.int32)[None, :]).astype(jnp.int32)
    before = jnp.cumsum(onehot, axis=0) - onehot
    return (flat_ids * CAP + lax.optimization_barrier(jnp.sum(before * onehot, axis=1))).astype(jnp.int32)

def slot_table(block_targets):
    pair_token = (jnp.arange(block_targets.shape[0], dtype=jnp.int32) // TOPK).astype(jnp.int32)
    slot_token = jnp.zeros((EXPERTS * CAP,), jnp.int32).at[block_targets].set(pair_token)
    slot_live = jnp.zeros((EXPERTS * CAP,), jnp.int32).at[block_targets].set(1)
    return (slot_token, slot_live)

def attention(query_rows, key_rows, value_rows, sink_logits):
    tok_total = query_rows.shape[0]
    queries = query_rows.reshape(tok_total, KV_HEADS, REP, HEAD_DIM)
    key_heads = jnp.pad(key_rows.reshape(tok_total, KV_HEADS, HEAD_DIM), ((WINDOW, 0), (0, 0), (0, 0)))
    value_heads = jnp.pad(value_rows.reshape(tok_total, KV_HEADS, HEAD_DIM), ((WINDOW, 0), (0, 0), (0, 0)))
    block_rows = TOK_SP
    sink_col = sink_logits.astype(jnp.float32).reshape(KV_HEADS, REP, 1, 1)

    def one_block(first_row):
        query_block = lax.dynamic_slice_in_dim(queries, first_row, block_rows, 0).astype(jnp.float32)
        key_block = lax.dynamic_slice_in_dim(key_heads, first_row, block_rows + WINDOW, 0).astype(jnp.float32)
        value_block = lax.dynamic_slice_in_dim(value_heads, first_row, block_rows + WINDOW, 0).astype(jnp.float32)
        query_pos = first_row + jnp.arange(block_rows, dtype=jnp.int32)
        key_pos = first_row - WINDOW + jnp.arange(block_rows + WINDOW, dtype=jnp.int32)
        distance = query_pos[:, None] - key_pos[None, :]
        allowed = (distance >= 0) & (distance < WINDOW) & (key_pos >= 0)[None, :]
        scores = jnp.einsum('qgrd,kgd->grqk', query_block, key_block) * HEAD_DIM ** (-0.5)
        scores = jnp.where(allowed[None, None], scores, -1e+30)
        row_peak = jnp.maximum(lax.optimization_barrier(jnp.max(scores, axis=-1, keepdims=True)), sink_col)
        exp_terms = jnp.exp(scores - row_peak)
        denom_sum = lax.optimization_barrier(jnp.sum(exp_terms, axis=-1, keepdims=True)) + jnp.exp(sink_col - row_peak)
        attn_probs = (exp_terms / denom_sum).astype(jnp.bfloat16)
        attended = jnp.einsum('grqk,kgd->qgrd', attn_probs.astype(jnp.float32), value_block)
        return attended.astype(jnp.bfloat16).reshape(block_rows, HEADS * HEAD_DIM)
    starts = jnp.arange(tok_total // block_rows, dtype=jnp.int32) * block_rows
    return lax.map(one_block, starts).reshape(tok_total, HEADS * HEAD_DIM)

def reference(query_rows, key_rows, value_rows, sink_logits, out_weight, stream_in, norm_gain, routes, route_weights, gate_weight, up_weight, down_weight):
    attended = attention(query_rows, key_rows, value_rows, sink_logits)
    head_cols = HEADS * HEAD_DIM // N_TP

    def add_group(group_index, running):
        first_col = (jnp.asarray(group_index) * head_cols).astype(jnp.int32)
        piece = lax.dynamic_slice_in_dim(attended, first_col, head_cols, 1)
        weight_piece = lax.dynamic_slice_in_dim(out_weight, first_col, head_cols, 0)
        partial_value = jnp.dot(piece, weight_piece, preferred_element_type=jnp.float32).astype(jnp.bfloat16)
        return running + lax.optimization_barrier(partial_value).astype(jnp.float32)
    projected = lax.fori_loop(0, N_TP, add_group, jnp.zeros((TOKENS, D), jnp.float32))
    stream = (stream_in.astype(jnp.float32) + projected).astype(jnp.bfloat16)
    values = stream.astype(jnp.float32)
    normed = (values * lax.rsqrt(lax.optimization_barrier(jnp.mean(values * values, axis=-1, keepdims=True)) + norm_eps) * norm_gain.astype(jnp.float32)).astype(jnp.bfloat16)
    targets = jax.vmap(route_targets)(routes.reshape(N_SP, TOK_SP, TOPK))
    slot_token, slot_live = jax.vmap(slot_table)(targets)
    slot_token = slot_token + (jnp.arange(N_SP, dtype=jnp.int32) * TOK_SP)[:, None]
    table_tokens = jnp.transpose(slot_token.reshape(N_SP, EXPERTS, CAP), (1, 0, 2))
    table_live = jnp.transpose(slot_live.reshape(N_SP, EXPERTS, CAP), (1, 0, 2))
    ff_cols = EXPERT_FF // N_TP

    def one_expert(inputs):
        expert_id, token_ids, live_ids = inputs
        rows_in = jnp.where(live_ids[..., None] > 0, normed[token_ids], jnp.zeros((), jnp.bfloat16))
        flat_rows = rows_in.reshape(N_SP * CAP, D)
        gate_act = jnp.dot(flat_rows, gate_weight[expert_id], preferred_element_type=jnp.float32)
        up_act = jnp.dot(flat_rows, up_weight[expert_id], preferred_element_type=jnp.float32)
        hidden = (jax.nn.silu(gate_act) * up_act).astype(jnp.bfloat16)
        down_full = down_weight[expert_id]

        def add_part(group_index, running):
            first_col = (jnp.asarray(group_index) * ff_cols).astype(jnp.int32)
            piece = lax.dynamic_slice_in_dim(hidden, first_col, ff_cols, 1)
            weight_piece = lax.dynamic_slice_in_dim(down_full, first_col, ff_cols, 0)
            partial_value = jnp.dot(piece, weight_piece, preferred_element_type=jnp.float32).astype(jnp.bfloat16)
            return running + lax.optimization_barrier(partial_value).astype(jnp.float32)
        summed = lax.fori_loop(0, N_TP, add_part, jnp.zeros((N_SP * CAP, D), jnp.float32))
        return summed.reshape(N_SP, CAP, D)
    expert_out = lax.map(one_expert, (jnp.arange(EXPERTS, dtype=jnp.int32), table_tokens, table_live))
    by_block = jnp.transpose(expert_out, (1, 0, 2, 3)).reshape(N_SP, EXPERTS * CAP, D)
    picked = jnp.take_along_axis(by_block, targets[:, :, None], axis=1)
    weighted = picked * route_weights.astype(jnp.float32).reshape(N_SP, TOK_SP * TOPK)[:, :, None]
    moe = lax.optimization_barrier(jnp.sum(weighted.reshape(N_SP, TOK_SP, TOPK, D), axis=2)).reshape(TOKENS, D)
    return (stream.astype(jnp.float32) + moe).astype(jnp.bfloat16)
```

```python
import jax
import jax.numpy as jnp
from jax import lax
from jax.sharding import Mesh
from jax.sharding import PartitionSpec as P

HEAD_DIM = 64
REP = 8
WINDOW = 128
TP = ("tp_0", "tp_1")
SP_TP = ("sp", "tp_0", "tp_1")


norm_eps = 1e-06


def shifted(block, axis, distance):
    devices = range(lax.axis_size(axis))
    route = [(i - distance, i) for i in devices if i - distance in devices]
    return lax.ppermute(block, axis, route)


def cut_along(shard, dim, count):
    before, after = (shard.shape[:dim], shard.shape[dim + 1 :])
    return jnp.moveaxis(shard.reshape(*before, count, -1, *after), dim, 0)


def sum_at_owner(shard, axis, dim):
    pieces = cut_along(shard, dim, lax.axis_size(axis))
    arrived = lax.all_to_all(pieces, axis, split_axis=0, concat_axis=0, tiled=True)
    return arrived.astype(jnp.float32).sum(axis=0)


def laid_out(pieces, dim):
    lengths = list(pieces.shape[1:])
    lengths[dim] *= pieces.shape[0]
    return jnp.moveaxis(pieces, 0, dim).reshape(lengths)


def sent_to_all(shard, axis):
    copies = jnp.broadcast_to(shard, (lax.axis_size(axis), *shard.shape))
    return lax.all_to_all(copies, axis, split_axis=0, concat_axis=0, tiled=True)


def gathered_copies(shard, axis, dim):
    return laid_out(sent_to_all(shard, axis), dim)


def gathered_by_axis(shard, axes, dim):
    result = shard
    for number in range(len(axes) - 1, -1, -1):
        result = lax.all_gather(result, axes[number], axis=dim, tiled=True)
    return result


def piece_ends(length, count):
    hop = length // count
    if hop >= 8:
        hop -= hop % 8
    return [hop * k for k in range(1, count)]


def exchange_in_pieces(shard, axis, pieces, split_dim, concat_dim):
    blocks = cut_along(shard, split_dim, lax.axis_size(axis))
    split_at = max(range(1, max(2, blocks.ndim - 1)), key=lambda d: blocks.shape[d])
    finished = []
    for slab in jnp.split(blocks, piece_ends(blocks.shape[split_at], pieces), axis=split_at):
        if slab.size:
            finished.append(lax.all_to_all(slab, axis, split_axis=0, concat_axis=0, tiled=True))
    return laid_out(jnp.concatenate(finished, axis=split_at), concat_dim)


def rms_scale(stream, norm_gain):
    values = stream.astype(jnp.float32)
    scaled = values * lax.rsqrt(jnp.mean(values * values, axis=-1, keepdims=True) + norm_eps)
    return (scaled * norm_gain).astype(jnp.bfloat16)


def slot_tables(routes, experts_n, slot_cap):
    flat_ids = routes.reshape(-1)
    onehot = (flat_ids[:, None] == jnp.arange(experts_n, dtype=jnp.int32)[None, :]).astype(
        jnp.int32
    )
    before = jnp.cumsum(onehot, axis=0) - onehot
    targets = flat_ids * slot_cap + jnp.sum(before * onehot, axis=1)
    pair_token = jnp.arange(flat_ids.shape[0], dtype=jnp.int32) // routes.shape[1]
    slot_token = jnp.zeros((experts_n * slot_cap,), jnp.int32).at[targets].set(pair_token)
    slot_live = jnp.zeros((experts_n * slot_cap,), jnp.int32).at[targets].set(1)
    return (targets, slot_token, slot_live)


def per_device(
    query_rows,
    key_rows,
    value_rows,
    sink_logits,
    out_weight,
    stream_in,
    norm_gain,
    routes,
    route_weights,
    gate_weight,
    up_weight,
    down_weight,
):
    tok_count = query_rows.shape[0]
    local_heads = query_rows.shape[1] // HEAD_DIM
    tp_index = lax.axis_index(TP)
    kv_group = tp_index * local_heads // REP
    own_keys = lax.dynamic_slice_in_dim(key_rows, kv_group * HEAD_DIM, HEAD_DIM, 1)
    own_values = lax.dynamic_slice_in_dim(value_rows, kv_group * HEAD_DIM, HEAD_DIM, 1)
    prior_keys, prior_values = shifted(
        (own_keys[tok_count - WINDOW :], own_values[tok_count - WINDOW :]), "sp", 1
    )
    key_block = jnp.concatenate([prior_keys, own_keys], axis=0)
    value_block = jnp.concatenate([prior_values, own_values], axis=0)
    offset = lax.axis_index("sp") * tok_count
    query_pos = offset + jnp.arange(tok_count, dtype=jnp.int32)
    key_pos = offset - WINDOW + jnp.arange(tok_count + WINDOW, dtype=jnp.int32)
    distance = query_pos[:, None] - key_pos[None, :]
    allowed = (distance >= 0) & (distance < WINDOW) & (key_pos >= 0)[None, :]
    queries = query_rows.reshape(tok_count, local_heads, HEAD_DIM)
    scores = jnp.einsum(
        "qhd,kd->hqk", queries, key_block, preferred_element_type=jnp.float32
    ) * HEAD_DIM ** (-0.5)
    scores = jnp.where(allowed[None], scores, -1e30)
    sink_col = sink_logits.reshape(local_heads, 1, 1)
    row_peak = jnp.maximum(jnp.max(scores, axis=-1, keepdims=True), sink_col)
    exp_terms = jnp.exp(scores - row_peak)
    denom_sum = jnp.sum(exp_terms, axis=-1, keepdims=True) + jnp.exp(sink_col - row_peak)
    attn_probs = (exp_terms / denom_sum).astype(jnp.bfloat16)
    attended = jnp.einsum(
        "hqk,kd->qhd", attn_probs, value_block, preferred_element_type=jnp.float32
    )
    attended = attended.astype(jnp.bfloat16).reshape(tok_count, local_heads * HEAD_DIM)
    width = out_weight.shape[1]
    width_share = width // lax.axis_size(TP)
    projected = sum_at_owner(
        jnp.dot(attended, out_weight, preferred_element_type=jnp.float32).astype(jnp.bfloat16),
        TP,
        1,
    )
    own_input = lax.dynamic_slice_in_dim(stream_in, tp_index * width_share, width_share, 1)
    columns = (own_input.astype(jnp.float32) + projected).astype(jnp.bfloat16)
    experts_n = lax.axis_size("sp")
    top_count = routes.shape[1]
    slot_cap = 3 * tok_count * top_count // (2 * experts_n)
    targets, slot_token, slot_live = slot_tables(routes, experts_n, slot_cap)
    outgoing = jnp.where(slot_live[:, None] > 0, columns[slot_token], jnp.zeros((), jnp.bfloat16))
    outgoing = outgoing.reshape(experts_n, slot_cap, width_share)
    arrived = lax.all_to_all(outgoing, "sp", split_axis=0, concat_axis=0, tiled=True)
    arrived = rms_scale(gathered_copies(arrived, TP, 2), norm_gain)
    sources = arrived.shape[0]
    item_count = arrived.shape[1]
    flat_rows = arrived.reshape(sources * item_count, arrived.shape[2])
    gate_act = jnp.dot(flat_rows, gate_weight[0], preferred_element_type=jnp.float32)
    up_act = jnp.dot(flat_rows, up_weight[0], preferred_element_type=jnp.float32)
    hidden = (jax.nn.silu(gate_act) * up_act).astype(jnp.bfloat16)
    partial_value = jnp.dot(hidden, down_weight[0], preferred_element_type=jnp.float32).astype(
        jnp.bfloat16
    )
    pieces = exchange_in_pieces(partial_value[None], TP, 1, 2, 0)
    summed = jnp.sum(pieces.astype(jnp.float32), axis=0)
    summed = summed.reshape(sources, item_count, summed.shape[1])
    returned = lax.all_to_all(
        summed.astype(jnp.bfloat16), "sp", split_axis=0, concat_axis=0, tiled=True
    ).astype(summed.dtype)
    returned_flat = returned.reshape(experts_n * slot_cap, returned.shape[2])
    pair_weights = route_weights.reshape(-1)
    chosen = returned_flat[targets] * pair_weights[:, None]
    moe_columns = jnp.sum(chosen.reshape(tok_count, top_count, chosen.shape[1]), axis=1)
    out_columns = (columns.astype(jnp.float32) + moe_columns).astype(jnp.bfloat16)
    return lax.all_to_all(out_columns, TP, split_axis=0, concat_axis=1, tiled=True)


def solution(mesh):
    finer = Mesh(mesh.devices.reshape(mesh.shape["sp"], 4, 4), ("sp", "tp_0", "tp_1"))
    placed = (
        P("sp", TP),
        P("sp", None),
        P("sp", None),
        P(TP),
        P(TP, None),
        P("sp", None),
        P(),
        P("sp", None),
        P("sp", None),
        P("sp", None, TP),
        P("sp", None, TP),
        P("sp", TP, None),
    )
    return jax.shard_map(
        per_device, mesh=finer, in_specs=placed, out_specs=P(SP_TP, None), check_vma=False
    )
```

```python
import functools

import jax
import jax.numpy as jnp
from jax import lax
from jax.experimental import pallas as pl
from jax.experimental.pallas import tpu as pltpu
from jax.sharding import Mesh
from jax.sharding import PartitionSpec as P

HEAD_DIM = 64
REP = 8
WINDOW = 128
LANES = 128
TP = ("tp_0", "tp_1")
SP_TP = ("sp", "tp_0", "tp_1")
NORM_EPS = 1e-06
BF16 = jnp.bfloat16
F32 = jnp.float32
VMEM_SPEC = pl.BlockSpec(memory_space=pltpu.VMEM)
SMEM_SPEC = pl.BlockSpec(memory_space=pltpu.SMEM)


def dot(a, b, contract=(1, 0)):
    return lax.dot_general(a, b, (((contract[0],), (contract[1],)), ((), ())), preferred_element_type=F32)


def head_pair(block, half):
    swapped = jnp.concatenate([block[:, HEAD_DIM:], block[:, :HEAD_DIM]], axis=1)
    lane = lax.broadcasted_iota(jnp.int32, block.shape, 1)
    low = jnp.where(half == 0, block, swapped)
    high = jnp.where(half == 0, swapped, block)
    zero = jnp.zeros_like(block)
    return jnp.where(lane < HEAD_DIM, low, zero), jnp.where(lane >= HEAD_DIM, high, zero)


def attention_body(place, sinks, q_ref, k_ref, v_ref, before_ref, w_ref, out_ref):
    first_block = place[0] == 0
    group = place[1]
    half = group % 2
    pair = group // 2
    pairs = k_ref.shape[1] // LANES

    def chosen(ref, row0, rows, col0):
        picked = ref[row0 : row0 + rows, col0 : col0 + LANES]
        for i in range(1, pairs):
            picked = jnp.where(pair == i, ref[row0 : row0 + rows, col0 + i * LANES : col0 + (i + 1) * LANES], picked)
        return picked.astype(F32)

    rows = q_ref.shape[0]
    width = k_ref.shape[1]
    keys = jnp.concatenate([chosen(before_ref, 0, WINDOW, 0), chosen(k_ref, 0, rows, 0)], axis=0)
    values = jnp.concatenate([chosen(before_ref, 0, WINDOW, width), chosen(v_ref, 0, rows, 0)], axis=0)
    keys = [k.astype(BF16) for k in head_pair(keys, half)]
    values = [v.astype(BF16) for v in head_pair(values, half)]
    row = lax.broadcasted_iota(jnp.int32, (WINDOW, 2 * WINDOW), 0)
    col = lax.broadcasted_iota(jnp.int32, (WINDOW, 2 * WINDOW), 1)
    inside = (col > row) & (col <= row + WINDOW)
    parts = []
    for block in range(rows // WINDOW):
        lo = block * WINDOW
        allowed = inside
        if block == 0:
            allowed = inside & ((col >= WINDOW) | jnp.logical_not(first_block))
        q = q_ref[lo : lo + WINDOW, :]
        total = None
        for h in range(2):
            scores = dot(q, keys[h][lo : lo + 2 * WINDOW], (1, 1)) * HEAD_DIM**-0.5
            scores = jnp.where(allowed, scores, -1e30)
            sink = sinks[h]
            peak = jnp.maximum(jnp.max(scores, axis=-1, keepdims=True), sink)
            terms = jnp.exp(scores - peak)
            total_terms = jnp.sum(terms, axis=-1, keepdims=True) + jnp.exp(sink - peak)
            probs = (terms / total_terms).astype(BF16)
            part = dot(probs, values[h][lo : lo + 2 * WINDOW])
            total = part if total is None else total + part
        parts.append(total.astype(BF16))
    attended = jnp.concatenate(parts, axis=0)
    for t in range(out_ref.shape[0]):
        out_ref[t] = dot(attended, w_ref[:, t * LANES : (t + 1) * LANES]).astype(BF16)


def attention(place, sinks, q, k, v, before, w):
    shares = w.shape[1] // LANES
    return pl.pallas_call(
        attention_body,
        out_shape=jax.ShapeDtypeStruct((shares, q.shape[0], LANES), BF16),
        in_specs=[SMEM_SPEC, SMEM_SPEC] + [VMEM_SPEC] * 5,
        out_specs=VMEM_SPEC,
        name="attention",
    )(place, sinks, q, k, v, before, w)


def slots_body(cap, experts, routes_ref, wide_ref, send_ref, take_ref):
    tokens = routes_ref.shape[0]
    slots = send_ref.shape[0]
    lane = lax.broadcasted_iota(jnp.int32, (tokens, LANES), 1)
    picks = [routes_ref[:, k : k + 1] for k in range(2)]
    hot = [(picks[k] == lane).astype(F32) for k in range(2)]
    r = lax.broadcasted_iota(jnp.int32, (tokens, tokens), 0)
    c = lax.broadcasted_iota(jnp.int32, (tokens, tokens), 1)
    ahead = dot((c < r).astype(BF16), (hot[0] + hot[1]).astype(BF16))
    slot_lane = lax.broadcasted_iota(jnp.int32, (tokens, slots), 1)
    for k in range(2):
        rank = jnp.sum(ahead * hot[k], axis=1, keepdims=True).astype(jnp.int32)
        target = picks[k] * cap + rank
        take_ref[k * tokens : (k + 1) * tokens, :] = (slot_lane == target).astype(F32).astype(BF16)
    sub = lax.broadcasted_iota(jnp.int32, (experts, tokens), 0)
    picks_w = [wide_ref[k : k + 1, :] for k in range(2)]
    hot_w = [(picks_w[k] == sub).astype(F32) for k in range(2)]
    ahead_w = dot((hot_w[0] + hot_w[1]).astype(BF16), (r < c).astype(BF16))
    slot_sub = lax.broadcasted_iota(jnp.int32, (slots, tokens), 0)
    hit = None
    for k in range(2):
        rank = jnp.sum(ahead_w * hot_w[k], axis=0, keepdims=True).astype(jnp.int32)
        target = picks_w[k] * cap + rank
        here = slot_sub == target
        hit = here if hit is None else hit | here
    send_ref[...] = hit.astype(F32).astype(BF16)


def slot_matrices(routes, experts, cap):
    tokens = routes.shape[0]
    slots = experts * cap
    return pl.pallas_call(
        functools.partial(slots_body, cap, experts),
        out_shape=(
            jax.ShapeDtypeStruct((slots, tokens), BF16),
            jax.ShapeDtypeStruct((2 * tokens, slots), BF16),
        ),
        in_specs=[VMEM_SPEC] * 2,
        out_specs=(VMEM_SPEC, VMEM_SPEC),
        name="slots",
    )(routes, routes.T)


def stream_body(place, arrived_ref, own_ref, send_ref, stream_ref, rows_ref):
    total = own_ref[...].astype(F32)
    summed = arrived_ref[0].astype(F32)
    for t in range(1, arrived_ref.shape[0]):
        summed = summed + arrived_ref[t].astype(F32)
    stream = (total + summed).astype(BF16)
    stream_ref[...] = stream
    rows_ref[...] = dot(send_ref[...], stream).astype(BF16)


def stream_and_rows(place, arrived, stream_in, send):
    tokens = stream_in.shape[0]
    slots = send.shape[0]
    return pl.pallas_call(
        stream_body,
        grid_spec=pltpu.PrefetchScalarGridSpec(
            num_scalar_prefetch=1,
            grid=(1,),
            in_specs=[
                pl.BlockSpec(arrived.shape, lambda i, place: (0, 0, 0)),
                pl.BlockSpec((tokens, LANES), lambda i, place: (0, place[2])),
                pl.BlockSpec(send.shape, lambda i, place: (0, 0)),
            ],
            out_specs=[
                pl.BlockSpec((tokens, LANES), lambda i, place: (0, 0)),
                pl.BlockSpec((slots, LANES), lambda i, place: (0, 0)),
            ],
        ),
        out_shape=(
            jax.ShapeDtypeStruct((tokens, LANES), BF16),
            jax.ShapeDtypeStruct((slots, LANES), BF16),
        ),
        name="stream",
    )(place, arrived, stream_in, send)


def expert_body(x_ref, gain_ref, gate_ref, up_ref, down_ref, out_ref):
    shares = x_ref.shape[0]
    stream = jnp.concatenate([x_ref[t] for t in range(shares)], axis=1).astype(F32)
    scale = lax.rsqrt(jnp.mean(stream * stream, axis=-1, keepdims=True) + NORM_EPS)
    normed = (stream * scale * gain_ref[...]).astype(BF16)
    gate_act = dot(normed, gate_ref[0])
    up_act = dot(normed, up_ref[0])
    hidden = (gate_act * jax.nn.sigmoid(gate_act) * up_act).astype(BF16)
    for t in range(shares):
        out_ref[t] = dot(hidden, down_ref[0, :, t * LANES : (t + 1) * LANES]).astype(BF16)


def expert(x, gain, gate, up, down, block):
    shares, rows, _ = x.shape
    step = pl.BlockSpec((shares, block, LANES), lambda i: (0, i, 0))

    def whole(a):
        return pl.BlockSpec(a.shape, lambda i: (0,) * a.ndim)

    return pl.pallas_call(
        expert_body,
        grid=(rows // block,),
        in_specs=[step, whole(gain), whole(gate), whole(up), whole(down)],
        out_specs=step,
        out_shape=jax.ShapeDtypeStruct(x.shape, BF16),
        name="expert",
    )(x, gain, gate, up, down)


def combine_body(rows_ref, take_ref, weights_ref, stream_ref, out_ref):
    tokens = stream_ref.shape[0]
    taken = dot(take_ref[...], rows_ref[...])
    moe = taken[:tokens] * weights_ref[:, 0:1] + taken[tokens:] * weights_ref[:, 1:2]
    out_ref[...] = (stream_ref[...].astype(F32) + moe).astype(BF16)


def combine(rows, take, weights, stream):
    return pl.pallas_call(
        combine_body,
        out_shape=jax.ShapeDtypeStruct(stream.shape, BF16),
        in_specs=[VMEM_SPEC] * 4,
        out_specs=VMEM_SPEC,
        name="combine",
    )(rows, take, weights, stream)


def per_device(
    query_rows,
    key_rows,
    value_rows,
    sink_logits,
    out_weight,
    stream_in,
    norm_gain,
    routes,
    route_weights,
    gate_weight,
    up_weight,
    down_weight,
):
    tokens = query_rows.shape[0]
    local_heads = query_rows.shape[1] // HEAD_DIM
    tp_size = lax.axis_size(TP)
    experts = lax.axis_size("sp")
    tp_index = lax.axis_index(TP)
    place = jnp.stack([lax.axis_index("sp"), tp_index * local_heads // REP, tp_index]).astype(jnp.int32)
    last = jnp.concatenate([key_rows[tokens - WINDOW :], value_rows[tokens - WINDOW :]], axis=1)
    before = lax.ppermute(last, "sp", [(i, i + 1) for i in range(experts - 1)])
    partial = attention(place, sink_logits, query_rows, key_rows, value_rows, before, out_weight)
    arrived = lax.all_to_all(partial, TP, split_axis=0, concat_axis=0, tiled=True)
    cap = 3 * tokens * routes.shape[1] // (2 * experts)
    send, take = slot_matrices(routes, experts, cap)
    stream, rows = stream_and_rows(place, arrived, stream_in, send)
    rows = lax.all_to_all(rows.reshape(experts, cap, LANES), "sp", split_axis=0, concat_axis=0, tiled=True)
    slots = experts * cap
    copies = jnp.broadcast_to(rows.reshape(slots, LANES), (tp_size, slots, LANES))
    features = lax.all_to_all(copies, TP, split_axis=0, concat_axis=0, tiled=True)
    parts = expert(features, norm_gain.reshape(1, -1), gate_weight, up_weight, down_weight, 192)
    parts = lax.all_to_all(parts, TP, split_axis=0, concat_axis=0, tiled=True)
    summed = jnp.sum(parts.astype(F32), axis=0).astype(BF16)
    returned = lax.all_to_all(summed.reshape(experts, cap, LANES), "sp", split_axis=0, concat_axis=0, tiled=True)
    out = combine(returned.reshape(slots, LANES), take, route_weights, stream)
    return lax.all_to_all(out, TP, split_axis=0, concat_axis=1, tiled=True)


def solution(mesh):
    finer = Mesh(mesh.devices.reshape(mesh.shape["sp"], 4, 4), ("sp", "tp_0", "tp_1"))
    placed = (
        P("sp", TP),
        P("sp", None),
        P("sp", None),
        P(TP),
        P(TP, None),
        P("sp", None),
        P(),
        P("sp", None),
        P("sp", None),
        P("sp", None, TP),
        P("sp", None, TP),
        P("sp", TP, None),
    )
    return jax.shard_map(
        per_device, mesh=finer, in_specs=placed, out_specs=P(SP_TP, None), check_vma=False
    )
```

```python
import functools

import jax
import jax.numpy as jnp
from jax import lax
from jax.experimental import pallas as pl
from jax.experimental.pallas import tpu as pltpu
from jax.sharding import Mesh
from jax.sharding import PartitionSpec as P

HEAD_DIM = 64
REP = 8
WINDOW = 128
LANES = 128
TP = ("tp_0", "tp_1")
SP_TP = ("sp", "tp_0", "tp_1")
NORM_EPS = 1e-06
BF16 = jnp.bfloat16
F32 = jnp.float32
VMEM_SPEC = pl.BlockSpec(memory_space=pltpu.VMEM)
SMEM_SPEC = pl.BlockSpec(memory_space=pltpu.SMEM)
PLANE = ("tp_1", "tp_0")
SIDE = 4
PIECES = 2


def in_vmem(*arrays):
    return [pltpu.with_memory_space_constraint(a, pltpu.VMEM) for a in arrays]


def vmem_out(shape):
    return pltpu.VMEM(shape, BF16)


def share_of(member, side):
    return member % side * side + member // side


def dot(a, b, contract=(1, 0)):
    return lax.dot_general(a, b, (((contract[0],), (contract[1],)), ((), ())), preferred_element_type=F32)


def head_pair(block, half):
    swapped = jnp.concatenate([block[:, HEAD_DIM:], block[:, :HEAD_DIM]], axis=1)
    lane = lax.broadcasted_iota(jnp.int32, block.shape, 1)
    low = jnp.where(half == 0, block, swapped)
    high = jnp.where(half == 0, swapped, block)
    zero = jnp.zeros_like(block)
    return jnp.where(lane < HEAD_DIM, low, zero), jnp.where(lane >= HEAD_DIM, high, zero)


def attention_body(place, sinks, q_ref, k_ref, v_ref, before_ref, w_ref, out_ref):
    first_block = place[0] == 0
    group = place[1]
    half = group % 2
    pair = group // 2
    pairs = k_ref.shape[1] // LANES

    def chosen(ref, row0, rows, col0):
        picked = ref[row0 : row0 + rows, col0 : col0 + LANES]
        for i in range(1, pairs):
            picked = jnp.where(pair == i, ref[row0 : row0 + rows, col0 + i * LANES : col0 + (i + 1) * LANES], picked)
        return picked.astype(F32)

    rows = q_ref.shape[0]
    width = k_ref.shape[1]
    keys = jnp.concatenate([chosen(before_ref, 0, WINDOW, 0), chosen(k_ref, 0, rows, 0)], axis=0)
    values = jnp.concatenate([chosen(before_ref, 0, WINDOW, width), chosen(v_ref, 0, rows, 0)], axis=0)
    keys = [k.astype(BF16) for k in head_pair(keys, half)]
    values = [v.astype(BF16) for v in head_pair(values, half)]
    row = lax.broadcasted_iota(jnp.int32, (WINDOW, 2 * WINDOW), 0)
    col = lax.broadcasted_iota(jnp.int32, (WINDOW, 2 * WINDOW), 1)
    inside = (col > row) & (col <= row + WINDOW)
    parts = []
    for block in range(rows // WINDOW):
        lo = block * WINDOW
        allowed = inside
        if block == 0:
            allowed = inside & ((col >= WINDOW) | jnp.logical_not(first_block))
        q = q_ref[lo : lo + WINDOW, :]
        total = None
        for h in range(2):
            scores = dot(q, keys[h][lo : lo + 2 * WINDOW], (1, 1)) * HEAD_DIM**-0.5
            scores = jnp.where(allowed, scores, -1e30)
            sink = sinks[h]
            peak = jnp.maximum(jnp.max(scores, axis=-1, keepdims=True), sink)
            terms = jnp.exp(scores - peak)
            total_terms = jnp.sum(terms, axis=-1, keepdims=True) + jnp.exp(sink - peak)
            probs = (terms / total_terms).astype(BF16)
            part = dot(probs, values[h][lo : lo + 2 * WINDOW])
            total = part if total is None else total + part
        parts.append(total.astype(BF16))
    attended = jnp.concatenate(parts, axis=0)
    for p in range(out_ref.shape[0]):
        t = share_of(p, SIDE)
        out_ref[p] = dot(attended, w_ref[:, t * LANES : (t + 1) * LANES]).astype(BF16)


def attention(place, sinks, q, k, v, before, w):
    shares = w.shape[1] // LANES
    return pl.pallas_call(
        attention_body,
        out_shape=vmem_out((shares, q.shape[0], LANES)),
        in_specs=[SMEM_SPEC, SMEM_SPEC] + [VMEM_SPEC] * 5,
        out_specs=VMEM_SPEC,
        compiler_params=pltpu.CompilerParams(vmem_limit_bytes=16 * 2**20),
        name="attention",
    )(place, sinks, q, k, v, *in_vmem(before), w)


def slots_body(cap, experts, routes_ref, wide_ref, send_ref, take_ref):
    tokens = routes_ref.shape[0]
    slots = send_ref.shape[0]
    lane = lax.broadcasted_iota(jnp.int32, (tokens, LANES), 1)
    picks = [routes_ref[:, k : k + 1] for k in range(2)]
    hot = [(picks[k] == lane).astype(F32) for k in range(2)]
    r = lax.broadcasted_iota(jnp.int32, (tokens, tokens), 0)
    c = lax.broadcasted_iota(jnp.int32, (tokens, tokens), 1)
    ahead = dot((c < r).astype(BF16), (hot[0] + hot[1]).astype(BF16))
    slot_lane = lax.broadcasted_iota(jnp.int32, (tokens, slots), 1)
    for k in range(2):
        rank = jnp.sum(ahead * hot[k], axis=1, keepdims=True).astype(jnp.int32)
        target = picks[k] * cap + rank
        take_ref[k * tokens : (k + 1) * tokens, :] = (slot_lane == target).astype(F32).astype(BF16)
    sub = lax.broadcasted_iota(jnp.int32, (experts, tokens), 0)
    picks_w = [wide_ref[k : k + 1, :] for k in range(2)]
    hot_w = [(picks_w[k] == sub).astype(F32) for k in range(2)]
    ahead_w = dot((hot_w[0] + hot_w[1]).astype(BF16), (r < c).astype(BF16))
    slot_sub = lax.broadcasted_iota(jnp.int32, (slots, tokens), 0)
    hit = None
    for k in range(2):
        rank = jnp.sum(ahead_w * hot_w[k], axis=0, keepdims=True).astype(jnp.int32)
        target = picks_w[k] * cap + rank
        here = slot_sub == target
        hit = here if hit is None else hit | here
    send_ref[...] = hit.astype(F32).astype(BF16)


def slot_matrices(routes, experts, cap):
    tokens = routes.shape[0]
    slots = experts * cap
    return pl.pallas_call(
        functools.partial(slots_body, cap, experts),
        out_shape=(
            vmem_out((slots, tokens)),
            vmem_out((2 * tokens, slots)),
        ),
        in_specs=[VMEM_SPEC] * 2,
        out_specs=(VMEM_SPEC, VMEM_SPEC),
        compiler_params=pltpu.CompilerParams(vmem_limit_bytes=16 * 2**20),
        name="slots",
    )(*in_vmem(routes, routes.T))


def stream_body(arrived_ref, own_ref, send_ref, stream_ref, rows_ref):
    summed = arrived_ref[0].astype(F32)
    for t in range(1, arrived_ref.shape[0]):
        summed = summed + arrived_ref[t].astype(F32)
    stream = (own_ref[...].astype(F32) + summed).astype(BF16)
    stream_ref[...] = stream
    rows_ref[...] = dot(send_ref[...], stream).astype(BF16)


def stream_and_rows(arrived, own, send):
    return pl.pallas_call(
        stream_body,
        out_shape=(vmem_out(own.shape), vmem_out((send.shape[0], LANES))),
        in_specs=[VMEM_SPEC] * 3,
        out_specs=(VMEM_SPEC, VMEM_SPEC),
        compiler_params=pltpu.CompilerParams(vmem_limit_bytes=16 * 2**20),
        name="stream",
    )(*in_vmem(arrived, own, send))


def expert_body(block, x_ref, gain_ref, gate_ref, up_ref, down_ref, out_ref):
    shares, rows, _ = x_ref.shape
    order = sorted(range(shares), key=lambda p: share_of(p, SIDE))
    for lo in range(0, rows, block):
        stream = jnp.concatenate([x_ref[p, lo : lo + block, :] for p in order], axis=1).astype(F32)
        scale = lax.rsqrt(jnp.mean(stream * stream, axis=-1, keepdims=True) + NORM_EPS)
        normed = (stream * scale * gain_ref[...]).astype(BF16)
        gate_act = dot(normed, gate_ref[0])
        up_act = dot(normed, up_ref[0])
        hidden = (gate_act * jax.nn.sigmoid(gate_act) * up_act).astype(BF16)
        for p in range(shares):
            t = share_of(p, SIDE)
            out_ref[p, lo : lo + block, :] = dot(hidden, down_ref[0, :, t * LANES : (t + 1) * LANES]).astype(BF16)


def expert(x, gain, gate, up, down, block):
    return pl.pallas_call(
        functools.partial(expert_body, block),
        out_shape=vmem_out(x.shape),
        in_specs=[VMEM_SPEC] * 5,
        out_specs=VMEM_SPEC,
        cost_estimate=pl.CostEstimate(flops=6 * x.shape[1] * gate.shape[1] * gate.shape[2], bytes_accessed=2 * x.size * 2, transcendentals=0),
        compiler_params=pltpu.CompilerParams(vmem_limit_bytes=24 * 2**20),
        name="expert",
    )(*in_vmem(x), gain, gate, up, down)


def combine_body(rows_ref, take_ref, weights_ref, stream_ref, out_ref):
    tokens = stream_ref.shape[0]
    taken = dot(take_ref[...], rows_ref[...])
    moe = taken[:tokens] * weights_ref[:, 0:1] + taken[tokens:] * weights_ref[:, 1:2]
    out_ref[...] = (stream_ref[...].astype(F32) + moe).astype(BF16)


def combine(rows, take, weights, stream):
    return pl.pallas_call(
        combine_body,
        out_shape=vmem_out(stream.shape),
        in_specs=[VMEM_SPEC] * 4,
        out_specs=VMEM_SPEC,
        compiler_params=pltpu.CompilerParams(vmem_limit_bytes=16 * 2**20),
        name="combine",
    )(*in_vmem(rows, take), weights, *in_vmem(stream))


def per_device(
    query_rows,
    key_rows,
    value_rows,
    sink_logits,
    out_weight,
    stream_in,
    norm_gain,
    routes,
    route_weights,
    gate_weight,
    up_weight,
    down_weight,
):
    tokens = query_rows.shape[0]
    local_heads = query_rows.shape[1] // HEAD_DIM
    tp_size = lax.axis_size(TP)
    experts = lax.axis_size("sp")
    tp_index = lax.axis_index(TP)
    place = jnp.stack([lax.axis_index("sp"), tp_index * local_heads // REP]).astype(jnp.int32)
    last = jnp.concatenate([key_rows[tokens - WINDOW :], value_rows[tokens - WINDOW :]], axis=1)
    before = lax.ppermute(last, "sp", [(i, i + 1) for i in range(experts - 1)])
    partial = attention(place, sink_logits, query_rows, key_rows, value_rows, before, out_weight)
    arrived = lax.all_to_all(partial, PLANE, split_axis=0, concat_axis=0, tiled=True)
    cap = 3 * tokens * routes.shape[1] // (2 * experts)
    send, take = slot_matrices(routes, experts, cap)
    own = lax.dynamic_slice_in_dim(stream_in, tp_index * LANES, LANES, 1)
    stream, rows = stream_and_rows(arrived, own, send)
    rows = lax.all_to_all(rows.reshape(experts, cap, LANES), "sp", split_axis=0, concat_axis=0, tiled=True)
    slots = experts * cap
    gain = norm_gain.reshape(1, -1)
    returned = []
    for piece in jnp.split(rows.reshape(slots, LANES), PIECES):
        copies = jnp.broadcast_to(piece, (tp_size, *piece.shape))
        features = lax.all_to_all(copies, PLANE, split_axis=0, concat_axis=0, tiled=True)
        parts = expert(features, gain, gate_weight, up_weight, down_weight, 192)
        parts = lax.all_to_all(parts, PLANE, split_axis=0, concat_axis=0, tiled=True)
        returned.append(jnp.sum(parts.astype(F32), axis=0).astype(BF16))
    returned = jnp.concatenate(returned, axis=0).reshape(experts, cap, LANES)
    returned = lax.all_to_all(returned, "sp", split_axis=0, concat_axis=0, tiled=True)
    out = combine(returned.reshape(slots, LANES), take, route_weights, stream)
    return lax.all_to_all(out, TP, split_axis=0, concat_axis=1, tiled=True)


def solution(mesh):
    finer = Mesh(mesh.devices.reshape(mesh.shape["sp"], 4, 4), ("sp", "tp_0", "tp_1"))
    placed = (
        P("sp", TP),
        P("sp", None),
        P("sp", None),
        P(TP),
        P(TP, None),
        P("sp", None),
        P(),
        P("sp", None),
        P("sp", None),
        P("sp", None, TP),
        P("sp", None, TP),
        P("sp", TP, None),
    )
    return jax.shard_map(
        per_device, mesh=finer, in_specs=placed, out_specs=P(SP_TP, None), check_vma=False
    )
```

```python
import functools

import jax
import jax.numpy as jnp
from jax import lax
from jax.experimental import pallas as pl
from jax.experimental.pallas import tpu as pltpu
from jax.sharding import Mesh
from jax.sharding import PartitionSpec as P

HEAD_DIM = 64
REP = 8
WINDOW = 128
LANES = 128
TP = ("tp_0", "tp_1")
SP_TP = ("sp", "tp_0", "tp_1")
NORM_EPS = 1e-06
BF16 = jnp.bfloat16
F32 = jnp.float32
VMEM_SPEC = pl.BlockSpec(memory_space=pltpu.VMEM)
SMEM_SPEC = pl.BlockSpec(memory_space=pltpu.SMEM)
PLANE = ("tp_1", "tp_0")
SIDE = 4
LAG_NS = 16000


def in_vmem(*arrays):
    return [pltpu.with_memory_space_constraint(a, pltpu.VMEM) for a in arrays]


def in_hbm(*arrays):
    return [pltpu.with_memory_space_constraint(a, pltpu.HBM) for a in arrays]


def small_kernel(mib):
    return pltpu.CompilerParams(vmem_limit_bytes=mib * 2**20)


def vmem_out(shape):
    return pltpu.VMEM(shape, BF16)


def share_of(member, side):
    return member % side * side + member // side


def dot(a, b, contract=(1, 0)):
    return lax.dot_general(a, b, (((contract[0],), (contract[1],)), ((), ())), preferred_element_type=F32)


def head_pair(block, half):
    swapped = jnp.concatenate([block[:, HEAD_DIM:], block[:, :HEAD_DIM]], axis=1)
    lane = lax.broadcasted_iota(jnp.int32, block.shape, 1)
    low = jnp.where(half == 0, block, swapped)
    high = jnp.where(half == 0, swapped, block)
    zero = jnp.zeros_like(block)
    return jnp.where(lane < HEAD_DIM, low, zero), jnp.where(lane >= HEAD_DIM, high, zero)


def attention_body(place, sinks, q_ref, k_ref, v_ref, before_ref, w_ref, out_ref):
    first_block = place[0] == 0
    group = place[1]
    half = group % 2
    pair = group // 2
    pairs = k_ref.shape[1] // LANES

    def chosen(ref, row0, rows, col0):
        picked = ref[row0 : row0 + rows, col0 : col0 + LANES]
        for i in range(1, pairs):
            picked = jnp.where(pair == i, ref[row0 : row0 + rows, col0 + i * LANES : col0 + (i + 1) * LANES], picked)
        return picked.astype(F32)

    rows = q_ref.shape[0]
    width = k_ref.shape[1]
    keys = jnp.concatenate([chosen(before_ref, 0, WINDOW, 0), chosen(k_ref, 0, rows, 0)], axis=0)
    values = jnp.concatenate([chosen(before_ref, 0, WINDOW, width), chosen(v_ref, 0, rows, 0)], axis=0)
    keys = [k.astype(BF16) for k in head_pair(keys, half)]
    values = [v.astype(BF16) for v in head_pair(values, half)]
    row = lax.broadcasted_iota(jnp.int32, (WINDOW, 2 * WINDOW), 0)
    col = lax.broadcasted_iota(jnp.int32, (WINDOW, 2 * WINDOW), 1)
    inside = (col > row) & (col <= row + WINDOW)
    parts = []
    for block in range(rows // WINDOW):
        lo = block * WINDOW
        allowed = inside
        if block == 0:
            allowed = inside & ((col >= WINDOW) | jnp.logical_not(first_block))
        q = q_ref[lo : lo + WINDOW, :]
        total = None
        for h in range(2):
            scores = dot(q, keys[h][lo : lo + 2 * WINDOW], (1, 1)) * HEAD_DIM**-0.5
            scores = jnp.where(allowed, scores, -1e30)
            sink = sinks[h]
            peak = jnp.maximum(jnp.max(scores, axis=-1, keepdims=True), sink)
            terms = jnp.exp(scores - peak)
            total_terms = jnp.sum(terms, axis=-1, keepdims=True) + jnp.exp(sink - peak)
            probs = (terms / total_terms).astype(BF16)
            part = dot(probs, values[h][lo : lo + 2 * WINDOW])
            total = part if total is None else total + part
        parts.append(total.astype(BF16))
    attended = jnp.concatenate(parts, axis=0)
    for p in range(out_ref.shape[0]):
        t = share_of(p, SIDE)
        out_ref[p] = dot(attended, w_ref[:, t * LANES : (t + 1) * LANES]).astype(BF16)


def attention(place, sinks, q, k, v, before, w):
    shares = w.shape[1] // LANES
    return pl.pallas_call(
        attention_body,
        out_shape=vmem_out((shares, q.shape[0], LANES)),
        in_specs=[SMEM_SPEC, SMEM_SPEC] + [VMEM_SPEC] * 5,
        out_specs=VMEM_SPEC,
        compiler_params=small_kernel(16),
        name="attention",
    )(place, *in_hbm(sinks, q, k, v), *in_vmem(before), *in_hbm(w))


def pack_body(k_ref, v_ref, out_ref):
    width = k_ref.shape[1]
    out_ref[:, :width] = k_ref[...]
    out_ref[:, width:] = v_ref[...]


def last_window(k, v):
    rows, width = k.shape
    tail = pl.BlockSpec((WINDOW, width), lambda i: (rows // WINDOW - 1, 0))
    return pl.pallas_call(
        pack_body,
        grid=(1,),
        out_shape=vmem_out((WINDOW, 2 * width)),
        in_specs=[tail, tail],
        out_specs=VMEM_SPEC,
        compiler_params=small_kernel(16),
        name="pack",
    )(*in_hbm(k, v))


def copies_body(place, rows_ref, out_ref):
    @pl.when(place[0] % 2 == 1)
    def _():
        pl.delay(LAG_NS)

    rows = rows_ref[...]
    for t in range(out_ref.shape[0]):
        out_ref[t] = rows


def copied(place, rows, count):
    return pl.pallas_call(
        copies_body,
        out_shape=vmem_out((count, *rows.shape)),
        in_specs=[SMEM_SPEC, VMEM_SPEC],
        out_specs=VMEM_SPEC,
        compiler_params=small_kernel(16),
        name="copies",
    )(place, *in_vmem(rows))


def total_body(parts_ref, out_ref):
    rows = parts_ref.shape[1]
    block = 128
    for lo in range(0, rows, block):
        summed = parts_ref[0, lo : lo + block, :].astype(F32)
        for t in range(1, parts_ref.shape[0]):
            summed = summed + parts_ref[t, lo : lo + block, :].astype(F32)
        out_ref[lo : lo + block, :] = summed.astype(BF16)


def total(parts):
    return pl.pallas_call(
        total_body,
        out_shape=vmem_out(parts.shape[1:]),
        in_specs=[VMEM_SPEC],
        out_specs=VMEM_SPEC,
        compiler_params=small_kernel(16),
        name="total",
    )(*in_vmem(parts))


def slots_body(cap, experts, routes_ref, wide_ref, send_ref, take_ref):
    tokens = routes_ref.shape[0]
    slots = send_ref.shape[0]
    lane = lax.broadcasted_iota(jnp.int32, (tokens, LANES), 1)
    picks = [routes_ref[:, k : k + 1] for k in range(2)]
    hot = [(picks[k] == lane).astype(F32) for k in range(2)]
    r = lax.broadcasted_iota(jnp.int32, (tokens, tokens), 0)
    c = lax.broadcasted_iota(jnp.int32, (tokens, tokens), 1)
    ahead = dot((c < r).astype(BF16), (hot[0] + hot[1]).astype(BF16))
    slot_lane = lax.broadcasted_iota(jnp.int32, (tokens, slots), 1)
    for k in range(2):
        rank = jnp.sum(ahead * hot[k], axis=1, keepdims=True).astype(jnp.int32)
        target = picks[k] * cap + rank
        take_ref[k * tokens : (k + 1) * tokens, :] = (slot_lane == target).astype(F32).astype(BF16)
    sub = lax.broadcasted_iota(jnp.int32, (experts, tokens), 0)
    picks_w = [wide_ref[k : k + 1, :] for k in range(2)]
    hot_w = [(picks_w[k] == sub).astype(F32) for k in range(2)]
    ahead_w = dot((hot_w[0] + hot_w[1]).astype(BF16), (r < c).astype(BF16))
    slot_sub = lax.broadcasted_iota(jnp.int32, (slots, tokens), 0)
    hit = None
    for k in range(2):
        rank = jnp.sum(ahead_w * hot_w[k], axis=0, keepdims=True).astype(jnp.int32)
        target = picks_w[k] * cap + rank
        here = slot_sub == target
        hit = here if hit is None else hit | here
    send_ref[...] = hit.astype(F32).astype(BF16)


def slot_matrices(routes, experts, cap):
    tokens = routes.shape[0]
    slots = experts * cap
    return pl.pallas_call(
        functools.partial(slots_body, cap, experts),
        out_shape=(
            vmem_out((slots, tokens)),
            vmem_out((2 * tokens, slots)),
        ),
        in_specs=[VMEM_SPEC] * 2,
        out_specs=(VMEM_SPEC, VMEM_SPEC),
        compiler_params=small_kernel(16),
        name="slots",
    )(*in_vmem(routes, routes.T))


def stream_body(arrived_ref, own_ref, send_ref, stream_ref, rows_ref):
    summed = arrived_ref[0].astype(F32)
    for t in range(1, arrived_ref.shape[0]):
        summed = summed + arrived_ref[t].astype(F32)
    stream = (own_ref[...].astype(F32) + summed).astype(BF16)
    stream_ref[...] = stream
    rows_ref[...] = dot(send_ref[...], stream).astype(BF16)


def stream_and_rows(arrived, own, send):
    return pl.pallas_call(
        stream_body,
        out_shape=(vmem_out(own.shape), vmem_out((send.shape[0], LANES))),
        in_specs=[VMEM_SPEC] * 3,
        out_specs=(VMEM_SPEC, VMEM_SPEC),
        compiler_params=small_kernel(16),
        name="stream",
    )(*in_vmem(arrived, own, send))


def expert_body(block, x_ref, gain_ref, gate_hbm, up_hbm, down_hbm, out_ref, gate_ref, up_ref, down_ref, sems):
    pairs = ((gate_hbm, gate_ref), (up_hbm, up_ref), (down_hbm, down_ref))
    copies = [pltpu.make_async_copy(source, target, sems.at[i]) for i, (source, target) in enumerate(pairs)]
    for copy in copies:
        copy.start()
    shares, rows, _ = x_ref.shape
    order = sorted(range(shares), key=lambda p: share_of(p, SIDE))
    for lo in range(0, rows, block):
        stream = jnp.concatenate([x_ref[p, lo : lo + block, :] for p in order], axis=1).astype(F32)
        scale = lax.rsqrt(jnp.mean(stream * stream, axis=-1, keepdims=True) + NORM_EPS)
        normed = (stream * scale * gain_ref[...]).astype(BF16)
        if lo == 0:
            copies[0].wait()
            copies[1].wait()
        gate_act = dot(normed, gate_ref[0])
        up_act = dot(normed, up_ref[0])
        hidden = (gate_act * jax.nn.sigmoid(gate_act) * up_act).astype(BF16)
        if lo == 0:
            copies[2].wait()
        for p in range(shares):
            t = share_of(p, SIDE)
            out_ref[p, lo : lo + block, :] = dot(hidden, down_ref[0, :, t * LANES : (t + 1) * LANES]).astype(BF16)


def expert(x, gain, gate, up, down, block):
    return pl.pallas_call(
        functools.partial(expert_body, block),
        out_shape=vmem_out(x.shape),
        in_specs=[VMEM_SPEC] * 2 + [pl.BlockSpec(memory_space=pltpu.HBM)] * 3,
        out_specs=VMEM_SPEC,
        scratch_shapes=[pltpu.VMEM(a.shape, BF16) for a in (gate, up, down)] + [pltpu.SemaphoreType.DMA((3,))],
        cost_estimate=pl.CostEstimate(flops=6 * x.shape[1] * gate.shape[1] * gate.shape[2], bytes_accessed=2 * x.size * 2, transcendentals=0),
        compiler_params=small_kernel(24),
        name="expert",
    )(*in_vmem(x, gain), *in_hbm(gate, up, down))


def combine_body(rows_ref, take_ref, weights_ref, stream_ref, out_ref):
    tokens = stream_ref.shape[0]
    taken = dot(take_ref[...], rows_ref[...])
    moe = taken[:tokens] * weights_ref[:, 0:1] + taken[tokens:] * weights_ref[:, 1:2]
    out_ref[...] = (stream_ref[...].astype(F32) + moe).astype(BF16)


def combine(rows, take, weights, stream):
    return pl.pallas_call(
        combine_body,
        out_shape=vmem_out(stream.shape),
        in_specs=[VMEM_SPEC] * 4,
        out_specs=VMEM_SPEC,
        compiler_params=small_kernel(16),
        name="combine",
    )(*in_vmem(rows, take), weights, *in_vmem(stream))


def per_device(
    query_rows,
    key_rows,
    value_rows,
    sink_logits,
    out_weight,
    stream_in,
    norm_gain,
    routes,
    route_weights,
    gate_weight,
    up_weight,
    down_weight,
):
    tokens = query_rows.shape[0]
    local_heads = query_rows.shape[1] // HEAD_DIM
    tp_size = lax.axis_size(TP)
    experts = lax.axis_size("sp")
    tp_index = lax.axis_index(TP)
    place = jnp.stack([lax.axis_index("sp"), tp_index * local_heads // REP]).astype(jnp.int32)
    last = last_window(key_rows, value_rows)
    before = lax.ppermute(last, "sp", [(i, i + 1) for i in range(experts - 1)])
    partial = attention(place, sink_logits, query_rows, key_rows, value_rows, before, out_weight)
    arrived = lax.all_to_all(partial, PLANE, split_axis=0, concat_axis=0, tiled=True)
    cap = 3 * tokens * routes.shape[1] // (2 * experts)
    send, take = slot_matrices(routes, experts, cap)
    own = lax.dynamic_slice_in_dim(stream_in, tp_index * LANES, LANES, 1)
    stream, rows = stream_and_rows(arrived, own, send)
    rows = lax.all_to_all(rows.reshape(experts, cap, LANES), "sp", split_axis=0, concat_axis=0, tiled=True)
    slots = experts * cap
    gain = norm_gain.reshape(1, -1)
    features = lax.all_to_all(copied(place, rows.reshape(slots, LANES), tp_size), PLANE, split_axis=0, concat_axis=0, tiled=True)
    parts = expert(features, gain, gate_weight, up_weight, down_weight, 192)
    summed = total(lax.all_to_all(parts, PLANE, split_axis=0, concat_axis=0, tiled=True))
    returned = lax.all_to_all(summed.reshape(experts, cap, LANES), "sp", split_axis=0, concat_axis=0, tiled=True)
    out = combine(returned.reshape(slots, LANES), take, route_weights, stream)
    return lax.all_to_all(out, TP, split_axis=0, concat_axis=1, tiled=True)


def solution(mesh):
    finer = Mesh(mesh.devices.reshape(mesh.shape["sp"], 4, 4), ("sp", "tp_0", "tp_1"))
    placed = (
        P("sp", TP),
        P("sp", None),
        P("sp", None),
        P(TP),
        P(TP, None),
        P("sp", None),
        P(),
        P("sp", None),
        P("sp", None),
        P("sp", None, TP),
        P("sp", None, TP),
        P("sp", TP, None),
    )
    return jax.shard_map(
        per_device, mesh=finer, in_specs=placed, out_specs=P(SP_TP, None), check_vma=False
    )
```

```python
import functools

import jax
import jax.numpy as jnp
from jax import lax
from jax.experimental import pallas as pl
from jax.experimental.pallas import tpu as pltpu
from jax.sharding import Mesh
from jax.sharding import PartitionSpec as P

HEAD_DIM = 64
REP = 8
WINDOW = 128
LANES = 128
TP = ("tp_0", "tp_1")
SP_TP = ("sp", "tp_0", "tp_1")
NORM_EPS = 1e-06
BF16 = jnp.bfloat16
F32 = jnp.float32
VMEM_SPEC = pl.BlockSpec(memory_space=pltpu.VMEM)
SMEM_SPEC = pl.BlockSpec(memory_space=pltpu.SMEM)
PLANE = ("tp_1", "tp_0")
SIDE = 4
LAG_NS = 17000


def in_vmem(*arrays):
    return [pltpu.with_memory_space_constraint(a, pltpu.VMEM) for a in arrays]


def in_hbm(*arrays):
    return [pltpu.with_memory_space_constraint(a, pltpu.HBM) for a in arrays]


def small_kernel(mib):
    return pltpu.CompilerParams(vmem_limit_bytes=mib * 2**20)


def vmem_out(shape):
    return pltpu.VMEM(shape, BF16)


def share_of(member, side):
    return member % side * side + member // side


def dot(a, b, contract=(1, 0)):
    return lax.dot_general(a, b, (((contract[0],), (contract[1],)), ((), ())), preferred_element_type=F32)


def both_places(block):
    swapped = jnp.concatenate([block[:, HEAD_DIM:], block[:, :HEAD_DIM]], axis=1)
    low = lax.broadcasted_iota(jnp.int32, block.shape, 1) < HEAD_DIM
    zero = jnp.zeros_like(block)
    keys = (jnp.where(low, block, zero), jnp.where(low, zero, swapped))
    values = (jnp.where(low, swapped, zero), jnp.where(low, zero, block))
    return [k.astype(BF16) for k in keys], [v.astype(BF16) for v in values]


def attend(q, keys, values, allowed, sinks):
    total = None
    for h in range(2):
        scores = dot(q, keys[h], (1, 1)) * HEAD_DIM**-0.5
        scores = jnp.where(allowed, scores, -1e30)
        sink = sinks[h]
        peak = jnp.maximum(jnp.max(scores, axis=-1, keepdims=True), sink)
        terms = jnp.exp(scores - peak)
        total_terms = jnp.sum(terms, axis=-1, keepdims=True) + jnp.exp(sink - peak)
        probs = (terms / total_terms).astype(BF16)
        part = dot(probs, values[h])
        total = part if total is None else total + part
    return total.astype(BF16)


def project(attended, w_ref, out_ref):
    for p in range(out_ref.shape[0]):
        t = share_of(p, SIDE)
        out_ref[p] = dot(attended, w_ref[:, t * LANES : (t + 1) * LANES]).astype(BF16)


def window_mask():
    row = lax.broadcasted_iota(jnp.int32, (WINDOW, 2 * WINDOW), 0)
    col = lax.broadcasted_iota(jnp.int32, (WINDOW, 2 * WINDOW), 1)
    return (col > row) & (col <= row + WINDOW), col


def later_body(sinks, q_ref, kv_ref, w_ref, out_ref):
    keys, values = both_places(kv_ref[...].astype(F32))
    inside, _ = window_mask()
    project(attend(q_ref[WINDOW:, :], keys, values, inside, sinks), w_ref, out_ref)


def first_body(place, sinks, q_ref, kv_ref, before_ref, w_ref, partial_ref, out_ref):
    keys, values = both_places(jnp.concatenate([before_ref[...], kv_ref[:WINDOW, :]], axis=0).astype(F32))
    inside, col = window_mask()
    allowed = inside & ((col >= WINDOW) | (place[0] > 0))
    project(attend(q_ref[:WINDOW, :], keys, values, allowed, sinks), w_ref, out_ref)


def half_out(shares, at):
    return pl.BlockSpec((shares, WINDOW, LANES), lambda i: (0, at, 0))


def attention_later(sinks, q, kv, w):
    shares = w.shape[1] // LANES
    return pl.pallas_call(
        later_body,
        grid=(1,),
        out_shape=pltpu.HBM((shares, q.shape[0], LANES), BF16),
        in_specs=[SMEM_SPEC] + [VMEM_SPEC] * 3,
        out_specs=half_out(shares, 1),
        compiler_params=small_kernel(16),
        cost_estimate=pl.CostEstimate(flops=10**9, bytes_accessed=2**20, transcendentals=2**16),
        name="attention_later",
    )(*in_hbm(sinks), *in_vmem(q, kv, w))


def attention_first(place, sinks, q, kv, before, w, partial):
    shares = w.shape[1] // LANES
    return pl.pallas_call(
        first_body,
        grid=(1,),
        out_shape=pltpu.HBM(partial.shape, BF16),
        in_specs=[SMEM_SPEC, SMEM_SPEC] + [VMEM_SPEC] * 4 + [pl.BlockSpec(memory_space=pltpu.HBM)],
        out_specs=half_out(shares, 0),
        input_output_aliases={6: 0},
        compiler_params=small_kernel(16),
        name="attention_first",
    )(place, *in_hbm(sinks), *in_vmem(q, kv, before, w), *in_hbm(partial))


def load_body(q_hbm, k_hbm, v_hbm, w_hbm, last_ref, kv_ref, q_ref, w_ref, k_ref, v_ref, sems):
    pairs = ((k_hbm, k_ref), (v_hbm, v_ref), (q_hbm, q_ref), (w_hbm, w_ref))
    copies = [pltpu.make_async_copy(source, target, sems.at[i]) for i, (source, target) in enumerate(pairs)]
    for copy in copies:
        copy.start()
    group = lax.axis_index(TP) * (q_ref.shape[1] // HEAD_DIM) // REP
    low = lax.broadcasted_iota(jnp.int32, kv_ref.shape, 1) < HEAD_DIM

    def head(ref):
        picked = ref[:, :LANES].astype(F32)
        for c in range(LANES, ref.shape[1], LANES):
            picked = jnp.where(group // 2 == c // LANES, ref[:, c : c + LANES].astype(F32), picked)
        return picked, jnp.concatenate([picked[:, HEAD_DIM:], picked[:, :HEAD_DIM]], axis=1)

    copies[0].wait()
    key, key_swapped = head(k_ref)
    copies[1].wait()
    value, value_swapped = head(v_ref)
    odd = group % 2 == 1
    kv = jnp.where(low, jnp.where(odd, key_swapped, key), jnp.where(odd, value, value_swapped)).astype(BF16)
    kv_ref[...] = kv
    last_ref[...] = kv[kv.shape[0] - WINDOW :]
    copies[2].wait()
    copies[3].wait()


def loaded(q, k, v, w):
    rows = q.shape[0]
    return pl.pallas_call(
        load_body,
        out_shape=(vmem_out((WINDOW, LANES)), vmem_out((rows, LANES)), vmem_out(q.shape), vmem_out(w.shape)),
        in_specs=[pl.BlockSpec(memory_space=pltpu.HBM)] * 4,
        out_specs=(VMEM_SPEC,) * 4,
        scratch_shapes=[pltpu.VMEM(k.shape, BF16), pltpu.VMEM(v.shape, BF16), pltpu.SemaphoreType.DMA((4,))],
        compiler_params=small_kernel(16),
        name="load",
    )(*in_hbm(q, k, v, w))


def copies_body(place, rows_ref, out_ref):
    @pl.when(place[0] % 2 == 1)
    def _():
        pl.delay(LAG_NS)

    rows = rows_ref[...]
    for t in range(out_ref.shape[0]):
        out_ref[t] = rows


def copied(place, rows, count):
    return pl.pallas_call(
        copies_body,
        out_shape=vmem_out((count, *rows.shape)),
        in_specs=[SMEM_SPEC, VMEM_SPEC],
        out_specs=VMEM_SPEC,
        compiler_params=small_kernel(16),
        name="copies",
    )(place, *in_vmem(rows))


def total_body(parts_ref, out_ref):
    rows = parts_ref.shape[1]
    block = 128
    for lo in range(0, rows, block):
        summed = parts_ref[0, lo : lo + block, :].astype(F32)
        for t in range(1, parts_ref.shape[0]):
            summed = summed + parts_ref[t, lo : lo + block, :].astype(F32)
        out_ref[lo : lo + block, :] = summed.astype(BF16)


def total(parts):
    return pl.pallas_call(
        total_body,
        out_shape=vmem_out(parts.shape[1:]),
        in_specs=[VMEM_SPEC],
        out_specs=VMEM_SPEC,
        compiler_params=small_kernel(16),
        name="total",
    )(*in_vmem(parts))


def slots_body(cap, experts, routes_ref, wide_ref, send_ref, take_ref):
    tokens = routes_ref.shape[0]
    slots = send_ref.shape[0]
    lane = lax.broadcasted_iota(jnp.int32, (tokens, LANES), 1)
    picks = [routes_ref[:, k : k + 1] for k in range(2)]
    hot = [(picks[k] == lane).astype(F32) for k in range(2)]
    r = lax.broadcasted_iota(jnp.int32, (tokens, tokens), 0)
    c = lax.broadcasted_iota(jnp.int32, (tokens, tokens), 1)
    ahead = dot((c < r).astype(BF16), (hot[0] + hot[1]).astype(BF16))
    slot_lane = lax.broadcasted_iota(jnp.int32, (tokens, slots), 1)
    for k in range(2):
        rank = jnp.sum(ahead * hot[k], axis=1, keepdims=True).astype(jnp.int32)
        target = picks[k] * cap + rank
        take_ref[k * tokens : (k + 1) * tokens, :] = (slot_lane == target).astype(F32).astype(BF16)
    sub = lax.broadcasted_iota(jnp.int32, (experts, tokens), 0)
    picks_w = [wide_ref[k : k + 1, :] for k in range(2)]
    hot_w = [(picks_w[k] == sub).astype(F32) for k in range(2)]
    ahead_w = dot((hot_w[0] + hot_w[1]).astype(BF16), (r < c).astype(BF16))
    slot_sub = lax.broadcasted_iota(jnp.int32, (slots, tokens), 0)
    hit = None
    for k in range(2):
        rank = jnp.sum(ahead_w * hot_w[k], axis=0, keepdims=True).astype(jnp.int32)
        target = picks_w[k] * cap + rank
        here = slot_sub == target
        hit = here if hit is None else hit | here
    send_ref[...] = hit.astype(F32).astype(BF16)


def slot_matrices(routes, experts, cap):
    tokens = routes.shape[0]
    slots = experts * cap
    return pl.pallas_call(
        functools.partial(slots_body, cap, experts),
        out_shape=(
            vmem_out((slots, tokens)),
            vmem_out((2 * tokens, slots)),
        ),
        in_specs=[VMEM_SPEC] * 2,
        out_specs=(VMEM_SPEC, VMEM_SPEC),
        compiler_params=small_kernel(16),
        name="slots",
    )(*in_vmem(routes, routes.T))


def stream_body(arrived_ref, own_ref, send_ref, stream_ref, rows_ref):
    summed = arrived_ref[0].astype(F32)
    for t in range(1, arrived_ref.shape[0]):
        summed = summed + arrived_ref[t].astype(F32)
    stream = (own_ref[...].astype(F32) + summed).astype(BF16)
    stream_ref[...] = stream
    rows_ref[...] = dot(send_ref[...], stream).astype(BF16)


def stream_and_rows(arrived, own, send):
    return pl.pallas_call(
        stream_body,
        out_shape=(vmem_out(own.shape), vmem_out((send.shape[0], LANES))),
        in_specs=[VMEM_SPEC] * 3,
        out_specs=(VMEM_SPEC, VMEM_SPEC),
        compiler_params=small_kernel(16),
        name="stream",
    )(*in_vmem(arrived, own, send))


def expert_body(block, x_ref, gain_ref, gate_ref, up_ref, down_ref, out_ref):
    shares, rows, _ = x_ref.shape
    order = sorted(range(shares), key=lambda p: share_of(p, SIDE))
    for lo in range(0, rows, block):
        stream = jnp.concatenate([x_ref[p, lo : lo + block, :] for p in order], axis=1).astype(F32)
        scale = lax.rsqrt(jnp.mean(stream * stream, axis=-1, keepdims=True) + NORM_EPS)
        normed = (stream * scale * gain_ref[...]).astype(BF16)
        gate_act = dot(normed, gate_ref[0])
        up_act = dot(normed, up_ref[0])
        hidden = (gate_act * jax.nn.sigmoid(gate_act) * up_act).astype(BF16)
        for p in range(shares):
            t = share_of(p, SIDE)
            out_ref[p, lo : lo + block, :] = dot(hidden, down_ref[0, :, t * LANES : (t + 1) * LANES]).astype(BF16)


def expert(x, gain, gate, up, down, block):
    return pl.pallas_call(
        functools.partial(expert_body, block),
        out_shape=vmem_out(x.shape),
        in_specs=[VMEM_SPEC] * 5,
        out_specs=VMEM_SPEC,
        cost_estimate=pl.CostEstimate(flops=6 * x.shape[1] * gate.shape[1] * gate.shape[2], bytes_accessed=2 * x.size * 2, transcendentals=0),
        compiler_params=small_kernel(24),
        name="expert",
    )(*in_vmem(x, gain, gate, up, down))


def combine_body(rows_ref, take_ref, weights_ref, stream_ref, out_ref):
    tokens = stream_ref.shape[0]
    taken = dot(take_ref[...], rows_ref[...])
    moe = taken[:tokens] * weights_ref[:, 0:1] + taken[tokens:] * weights_ref[:, 1:2]
    out_ref[...] = (stream_ref[...].astype(F32) + moe).astype(BF16)


def combine(rows, take, weights, stream):
    return pl.pallas_call(
        combine_body,
        out_shape=vmem_out(stream.shape),
        in_specs=[VMEM_SPEC] * 4,
        out_specs=VMEM_SPEC,
        compiler_params=small_kernel(16),
        name="combine",
    )(*in_vmem(rows, take), weights, *in_vmem(stream))


def per_device(
    query_rows,
    key_rows,
    value_rows,
    sink_logits,
    out_weight,
    stream_in,
    norm_gain,
    routes,
    route_weights,
    gate_weight,
    up_weight,
    down_weight,
):
    tokens = query_rows.shape[0]
    tp_size = lax.axis_size(TP)
    experts = lax.axis_size("sp")
    tp_index = lax.axis_index(TP)
    place = lax.axis_index("sp").reshape(1).astype(jnp.int32)
    last, kv, queries, out_share = loaded(query_rows, key_rows, value_rows, out_weight)
    before = lax.ppermute(last, "sp", [(i, i + 1) for i in range(experts - 1)])
    later = attention_later(sink_logits, queries, kv, out_share)
    partial = attention_first(place, sink_logits, queries, kv, before, out_share, later)
    arrived = lax.all_to_all(partial, PLANE, split_axis=0, concat_axis=0, tiled=True)
    cap = 3 * tokens * routes.shape[1] // (2 * experts)
    send, take = slot_matrices(routes, experts, cap)
    own = lax.dynamic_slice_in_dim(stream_in, tp_index * LANES, LANES, 1)
    stream, rows = stream_and_rows(arrived, own, send)
    rows = lax.all_to_all(rows.reshape(experts, cap, LANES), "sp", split_axis=0, concat_axis=0, tiled=True)
    slots = experts * cap
    gain = norm_gain.reshape(1, -1)
    copies = copied(place, rows.reshape(slots, LANES), tp_size)
    features = lax.all_to_all(copies, PLANE, split_axis=0, concat_axis=0, tiled=True)
    parts = expert(features, gain, gate_weight, up_weight, down_weight, 192)
    summed = total(lax.all_to_all(parts, PLANE, split_axis=0, concat_axis=0, tiled=True))
    returned = lax.all_to_all(summed.reshape(experts, cap, LANES), "sp", split_axis=0, concat_axis=0, tiled=True)
    out = combine(returned.reshape(slots, LANES), take, route_weights, stream)
    return lax.all_to_all(out, TP, split_axis=0, concat_axis=1, tiled=True)


def solution(mesh):
    finer = Mesh(mesh.devices.reshape(mesh.shape["sp"], 4, 4), ("sp", "tp_0", "tp_1"))
    placed = (
        P("sp", TP),
        P("sp", None),
        P("sp", None),
        P(TP),
        P(TP, None),
        P("sp", None),
        P(),
        P("sp", None),
        P("sp", None),
        P("sp", None, TP),
        P("sp", None, TP),
        P("sp", TP, None),
    )
    return jax.shard_map(
        per_device, mesh=finer, in_specs=placed, out_specs=P(SP_TP, None), check_vma=False
    )
```

```python
import functools

import jax
import jax.numpy as jnp
from jax import lax
from jax.experimental import pallas as pl
from jax.experimental.pallas import tpu as pltpu
from jax.sharding import Mesh
from jax.sharding import PartitionSpec as P

HEAD_DIM = 64
REP = 8
WINDOW = 128
LANES = 128
TP = ("tp_0", "tp_1")
SP_TP = ("sp", "tp_0", "tp_1")
NORM_EPS = 1e-06
BF16 = jnp.bfloat16
F32 = jnp.float32
VMEM_SPEC = pl.BlockSpec(memory_space=pltpu.VMEM)
LAG_NS = 17000


def in_vmem(*arrays):
    return [pltpu.with_memory_space_constraint(a, pltpu.VMEM) for a in arrays]


def in_hbm(*arrays):
    return [pltpu.with_memory_space_constraint(a, pltpu.HBM) for a in arrays]


def small_kernel(mib):
    return pltpu.CompilerParams(vmem_limit_bytes=mib * 2**20)


def vmem_out(shape):
    return pltpu.VMEM(shape, BF16)


def dot(a, b, contract=(1, 0)):
    return lax.dot_general(a, b, (((contract[0],), (contract[1],)), ((), ())), preferred_element_type=F32)


def both_places(block):
    swapped = jnp.concatenate([block[:, HEAD_DIM:], block[:, :HEAD_DIM]], axis=1)
    low = lax.broadcasted_iota(jnp.int32, block.shape, 1) < HEAD_DIM
    zero = jnp.zeros_like(block)
    keys = (jnp.where(low, block, zero), jnp.where(low, zero, swapped))
    values = (jnp.where(low, swapped, zero), jnp.where(low, zero, block))
    return [k.astype(BF16) for k in keys], [v.astype(BF16) for v in values]


def attend(q, keys, values, allowed, sinks):
    total = None
    for h in range(2):
        scores = dot(q, keys[h], (1, 1)) * HEAD_DIM**-0.5
        scores = jnp.where(allowed, scores, -1e30)
        sink = sinks[h : h + 1, :1]
        peak = jnp.maximum(jnp.max(scores, axis=-1, keepdims=True), sink)
        terms = jnp.exp(scores - peak)
        total_terms = jnp.sum(terms, axis=-1, keepdims=True) + jnp.exp(sink - peak)
        probs = (terms / total_terms).astype(BF16)
        part = dot(probs, values[h])
        total = part if total is None else total + part
    return total.astype(BF16)


def project(attended, w_ref, stage_ref, out_hbm, sems, row0):
    copies = []
    for j in range(stage_ref.shape[0] // 2):
        both = dot(attended, w_ref[:, 2 * j * LANES : 2 * (j + 1) * LANES]).astype(BF16)
        stage_ref[2 * j] = both[:, :LANES]
        stage_ref[2 * j + 1] = both[:, LANES:]
        pair = pl.ds(2 * j, 2)
        copy = pltpu.make_async_copy(stage_ref.at[pair], out_hbm.at[pair, pl.ds(row0, WINDOW), :], sems.at[j])
        copy.start()
        copies.append(copy)
    for copy in copies:
        copy.wait()


def window_mask():
    row = lax.broadcasted_iota(jnp.int32, (WINDOW, 2 * WINDOW), 0)
    col = lax.broadcasted_iota(jnp.int32, (WINDOW, 2 * WINDOW), 1)
    return (col > row) & (col <= row + WINDOW), col


def later_body(sinks_ref, q_ref, kv_ref, w_ref, out_hbm, stage_ref, sems):
    keys, values = both_places(kv_ref[...].astype(F32))
    inside, _ = window_mask()
    project(attend(q_ref[WINDOW:, :], keys, values, inside, sinks_ref[...]), w_ref, stage_ref, out_hbm, sems, WINDOW)


def first_body(sinks_ref, q_ref, kv_ref, before_ref, w_ref, partial_ref, out_hbm, stage_ref, sems):
    keys, values = both_places(jnp.concatenate([before_ref[...], kv_ref[:WINDOW, :]], axis=0).astype(F32))
    inside, col = window_mask()
    allowed = inside & ((col >= WINDOW) | (lax.axis_index("sp") > 0))
    project(attend(q_ref[:WINDOW, :], keys, values, allowed, sinks_ref[...]), w_ref, stage_ref, out_hbm, sems, 0)


def stages(shares):
    return [pltpu.VMEM((shares, WINDOW, LANES), BF16), pltpu.SemaphoreType.DMA((shares // 2,))]


def attention_later(sinks, q, kv, w):
    shares = w.shape[1] // LANES
    return pl.pallas_call(
        later_body,
        out_shape=pltpu.HBM((shares, q.shape[0], LANES), BF16),
        in_specs=[VMEM_SPEC] * 4,
        out_specs=pl.BlockSpec(memory_space=pltpu.HBM),
        scratch_shapes=stages(shares),
        compiler_params=small_kernel(16),
        cost_estimate=pl.CostEstimate(flops=10**9, bytes_accessed=2**20, transcendentals=2**16),
        name="attention_later",
    )(*in_vmem(sinks, q, kv, w))


def attention_first(sinks, q, kv, before, w, partial):
    shares = w.shape[1] // LANES
    return pl.pallas_call(
        first_body,
        out_shape=pltpu.HBM(partial.shape, BF16),
        in_specs=[VMEM_SPEC] * 5 + [pl.BlockSpec(memory_space=pltpu.HBM)],
        out_specs=pl.BlockSpec(memory_space=pltpu.HBM),
        scratch_shapes=stages(shares),
        input_output_aliases={5: 0},
        compiler_params=small_kernel(16),
        name="attention_first",
    )(*in_vmem(sinks, q, kv, before, w), *in_hbm(partial))


def load_body(sinks_hbm, q_hbm, k_hbm, v_hbm, w_hbm, last_ref, kv_ref, sinks_ref, q_ref, w_ref, k_ref, v_ref, sinks_smem, sems):
    pairs = ((k_hbm, k_ref), (v_hbm, v_ref), (q_hbm, q_ref), (w_hbm, w_ref), (sinks_hbm, sinks_smem))
    copies = [pltpu.make_async_copy(source, target, sems.at[i]) for i, (source, target) in enumerate(pairs)]
    for copy in copies:
        copy.start()
    group = lax.axis_index(TP) * (q_ref.shape[1] // HEAD_DIM) // REP
    low = lax.broadcasted_iota(jnp.int32, kv_ref.shape, 1) < HEAD_DIM

    def head(ref):
        picked = ref[:, :LANES].astype(F32)
        for c in range(LANES, ref.shape[1], LANES):
            picked = jnp.where(group // 2 == c // LANES, ref[:, c : c + LANES].astype(F32), picked)
        return picked, jnp.concatenate([picked[:, HEAD_DIM:], picked[:, :HEAD_DIM]], axis=1)

    copies[0].wait()
    key, key_swapped = head(k_ref)
    copies[1].wait()
    value, value_swapped = head(v_ref)
    odd = group % 2 == 1
    kv = jnp.where(low, jnp.where(odd, key_swapped, key), jnp.where(odd, value, value_swapped)).astype(BF16)
    kv_ref[...] = kv
    last_ref[...] = kv[kv.shape[0] - WINDOW :]
    copies[4].wait()
    row = lax.broadcasted_iota(jnp.int32, sinks_ref.shape, 0)
    sinks_ref[...] = jnp.where(row == 0, sinks_smem[0], sinks_smem[1])
    copies[2].wait()
    copies[3].wait()


def loaded(sinks, q, k, v, w):
    rows = q.shape[0]
    return pl.pallas_call(
        load_body,
        out_shape=(vmem_out((WINDOW, LANES)), vmem_out((rows, LANES)), pltpu.VMEM((8, LANES), F32), vmem_out(q.shape), vmem_out(w.shape)),
        in_specs=[pl.BlockSpec(memory_space=pltpu.HBM)] * 5,
        out_specs=(VMEM_SPEC,) * 5,
        scratch_shapes=[pltpu.VMEM(k.shape, BF16), pltpu.VMEM(v.shape, BF16), pltpu.SMEM(sinks.shape, F32), pltpu.SemaphoreType.DMA((5,))],
        compiler_params=small_kernel(16),
        name="load",
    )(*in_hbm(sinks, q, k, v, w))


def copies_body(rows_ref, out_ref):
    @pl.when(lax.axis_index("sp") % 2 == 1)
    def _():
        pl.delay(LAG_NS)

    rows = rows_ref[...]
    for t in range(out_ref.shape[0]):
        out_ref[t] = rows


def copied(rows, count):
    return pl.pallas_call(
        copies_body,
        out_shape=vmem_out((count, *rows.shape)),
        in_specs=[VMEM_SPEC],
        out_specs=VMEM_SPEC,
        compiler_params=small_kernel(16),
        name="copies",
    )(*in_vmem(rows))


def total_body(parts_ref, out_ref):
    rows = parts_ref.shape[1]
    block = 64
    for lo in range(0, rows, block):
        summed = parts_ref[0, lo : lo + block, :].astype(F32)
        for t in range(1, parts_ref.shape[0]):
            summed = summed + parts_ref[t, lo : lo + block, :].astype(F32)
        out_ref[lo : lo + block, :] = summed.astype(BF16)


def total(parts):
    return pl.pallas_call(
        total_body,
        out_shape=vmem_out(parts.shape[1:]),
        in_specs=[VMEM_SPEC],
        out_specs=VMEM_SPEC,
        compiler_params=small_kernel(16),
        name="total",
    )(*in_vmem(parts))


def slots_body(cap, experts, routes_ref, wide_ref, send_ref, take_ref):
    tokens = routes_ref.shape[0]
    slots = send_ref.shape[0]
    lane = lax.broadcasted_iota(jnp.int32, (tokens, LANES), 1)
    picks = [routes_ref[:, k : k + 1] for k in range(2)]
    hot = [(picks[k] == lane).astype(F32) for k in range(2)]
    r = lax.broadcasted_iota(jnp.int32, (tokens, tokens), 0)
    c = lax.broadcasted_iota(jnp.int32, (tokens, tokens), 1)
    ahead = dot((c < r).astype(BF16), (hot[0] + hot[1]).astype(BF16))
    slot_lane = lax.broadcasted_iota(jnp.int32, (tokens, slots), 1)
    for k in range(2):
        rank = jnp.sum(ahead * hot[k], axis=1, keepdims=True).astype(jnp.int32)
        target = picks[k] * cap + rank
        take_ref[k * tokens : (k + 1) * tokens, :] = (slot_lane == target).astype(F32).astype(BF16)
    sub = lax.broadcasted_iota(jnp.int32, (experts, tokens), 0)
    picks_w = [wide_ref[k : k + 1, :] for k in range(2)]
    hot_w = [(picks_w[k] == sub).astype(F32) for k in range(2)]
    ahead_w = dot((hot_w[0] + hot_w[1]).astype(BF16), (r < c).astype(BF16))
    slot_sub = lax.broadcasted_iota(jnp.int32, (slots, tokens), 0)
    hit = None
    for k in range(2):
        rank = jnp.sum(ahead_w * hot_w[k], axis=0, keepdims=True).astype(jnp.int32)
        target = picks_w[k] * cap + rank
        here = slot_sub == target
        hit = here if hit is None else hit | here
    send_ref[...] = hit.astype(F32).astype(BF16)


def slot_matrices(routes, experts, cap):
    tokens = routes.shape[0]
    slots = experts * cap
    return pl.pallas_call(
        functools.partial(slots_body, cap, experts),
        out_shape=(
            vmem_out((slots, tokens)),
            vmem_out((2 * tokens, slots)),
        ),
        in_specs=[VMEM_SPEC] * 2,
        out_specs=(VMEM_SPEC, VMEM_SPEC),
        compiler_params=small_kernel(16),
        name="slots",
    )(*in_vmem(routes, routes.T))


def stream_body(arrived_ref, own_ref, send_ref, stream_ref, rows_ref):
    summed = arrived_ref[0].astype(F32)
    for t in range(1, arrived_ref.shape[0]):
        summed = summed + arrived_ref[t].astype(F32)
    stream = (own_ref[...].astype(F32) + summed).astype(BF16)
    stream_ref[...] = stream
    rows_ref[...] = dot(send_ref[...], stream).astype(BF16)


def stream_and_rows(arrived, own, send):
    return pl.pallas_call(
        stream_body,
        out_shape=(vmem_out(own.shape), vmem_out((send.shape[0], LANES))),
        in_specs=[VMEM_SPEC] * 3,
        out_specs=(VMEM_SPEC, VMEM_SPEC),
        compiler_params=small_kernel(16),
        name="stream",
    )(*in_vmem(arrived, own, send))


def expert_body(block, x_ref, gain_ref, gate_ref, up_ref, down_ref, out_ref):
    shares, rows, _ = x_ref.shape
    for lo in range(0, rows, block):
        stream = jnp.concatenate([x_ref[t, lo : lo + block, :] for t in range(shares)], axis=1).astype(F32)
        scale = lax.rsqrt(jnp.mean(stream * stream, axis=-1, keepdims=True) + NORM_EPS)
        normed = (stream * scale * gain_ref[...]).astype(BF16)
        gate_act = dot(normed, gate_ref[0])
        up_act = dot(normed, up_ref[0])
        hidden = (gate_act * jax.nn.sigmoid(gate_act) * up_act).astype(BF16)
        for t in range(0, shares, 2):
            both = dot(hidden, down_ref[0, :, t * LANES : (t + 2) * LANES]).astype(BF16)
            out_ref[t, lo : lo + block, :] = both[:, :LANES]
            out_ref[t + 1, lo : lo + block, :] = both[:, LANES:]


def expert(x, gain, gate, up, down, block):
    return pl.pallas_call(
        functools.partial(expert_body, block),
        out_shape=vmem_out(x.shape),
        in_specs=[VMEM_SPEC] * 5,
        out_specs=VMEM_SPEC,
        cost_estimate=pl.CostEstimate(flops=6 * x.shape[1] * gate.shape[1] * gate.shape[2], bytes_accessed=2 * x.size * 2, transcendentals=0),
        compiler_params=small_kernel(24),
        name="expert",
    )(*in_vmem(x, gain, gate, up, down))


def combine_body(rows_ref, take_ref, weights_ref, stream_ref, out_ref):
    tokens = stream_ref.shape[0]
    taken = dot(take_ref[...], rows_ref[...])
    moe = taken[:tokens] * weights_ref[:, 0:1] + taken[tokens:] * weights_ref[:, 1:2]
    out_ref[...] = (stream_ref[...].astype(F32) + moe).astype(BF16)


def combine(rows, take, weights, stream):
    return pl.pallas_call(
        combine_body,
        out_shape=vmem_out(stream.shape),
        in_specs=[VMEM_SPEC] * 4,
        out_specs=VMEM_SPEC,
        compiler_params=small_kernel(16),
        name="combine",
    )(*in_vmem(rows, take), weights, *in_vmem(stream))


def per_device(
    query_rows,
    key_rows,
    value_rows,
    sink_logits,
    out_weight,
    stream_in,
    norm_gain,
    routes,
    route_weights,
    gate_weight,
    up_weight,
    down_weight,
):
    tokens = query_rows.shape[0]
    tp_size = lax.axis_size(TP)
    experts = lax.axis_size("sp")
    tp_index = lax.axis_index(TP)
    last, kv, sinks, queries, out_share = loaded(sink_logits, query_rows, key_rows, value_rows, out_weight)
    before = lax.ppermute(last, "sp", [(i, i + 1) for i in range(experts - 1)])
    later = attention_later(sinks, queries, kv, out_share)
    partial = attention_first(sinks, queries, kv, before, out_share, later)
    arrived = lax.all_to_all(partial, TP, split_axis=0, concat_axis=0, tiled=True)
    cap = 3 * tokens * routes.shape[1] // (2 * experts)
    send, take = slot_matrices(routes, experts, cap)
    own = lax.dynamic_slice_in_dim(stream_in, tp_index * LANES, LANES, 1)
    stream, rows = stream_and_rows(arrived, own, send)
    rows = lax.all_to_all(rows.reshape(experts, cap, LANES), "sp", split_axis=0, concat_axis=0, tiled=True)
    slots = experts * cap
    gain = norm_gain.reshape(1, -1)
    copies = copied(rows.reshape(slots, LANES), tp_size)
    features = lax.all_to_all(copies, TP, split_axis=0, concat_axis=0, tiled=True)
    parts = expert(features, gain, gate_weight, up_weight, down_weight, 384)
    summed = total(lax.all_to_all(parts, TP, split_axis=0, concat_axis=0, tiled=True))
    returned = lax.all_to_all(summed.reshape(experts, cap, LANES), "sp", split_axis=0, concat_axis=0, tiled=True)
    out = combine(returned.reshape(slots, LANES), take, route_weights, stream)
    return lax.all_to_all(out, TP, split_axis=0, concat_axis=1, tiled=True)


def solution(mesh):
    finer = Mesh(mesh.devices.reshape(mesh.shape["sp"], 4, 4), ("sp", "tp_0", "tp_1"))
    placed = (
        P("sp", TP),
        P("sp", None),
        P("sp", None),
        P(TP),
        P(TP, None),
        P("sp", None),
        P(),
        P("sp", None),
        P("sp", None),
        P("sp", None, TP),
        P("sp", None, TP),
        P("sp", TP, None),
    )
    return jax.shard_map(
        per_device, mesh=finer, in_specs=placed, out_specs=P(SP_TP, None), check_vma=False
    )
```

```python
import functools

import jax
import jax.numpy as jnp
from jax import lax
from jax.experimental import pallas as pl
from jax.experimental.pallas import tpu as pltpu
from jax.sharding import Mesh
from jax.sharding import PartitionSpec as P

HEAD_DIM = 64
REP = 8
WINDOW = 128
LANES = 128
TP = ("tp_0", "tp_1")
SP_TP = ("sp", "tp_0", "tp_1")
NORM_EPS = 1e-06
BF16 = jnp.bfloat16
F32 = jnp.float32
VMEM_SPEC = pl.BlockSpec(memory_space=pltpu.VMEM)
LAG_NS = 16500


def in_vmem(*arrays):
    return [pltpu.with_memory_space_constraint(a, pltpu.VMEM) for a in arrays]


def in_hbm(*arrays):
    return [pltpu.with_memory_space_constraint(a, pltpu.HBM) for a in arrays]


def small_kernel(mib):
    return pltpu.CompilerParams(vmem_limit_bytes=mib * 2**20)


def vmem_out(shape):
    return pltpu.VMEM(shape, BF16)


def dot(a, b, contract=(1, 0)):
    return lax.dot_general(a, b, (((contract[0],), (contract[1],)), ((), ())), preferred_element_type=F32)


def both_places(block):
    swapped = jnp.concatenate([block[:, HEAD_DIM:], block[:, :HEAD_DIM]], axis=1)
    low = lax.broadcasted_iota(jnp.int32, block.shape, 1) < HEAD_DIM
    zero = jnp.zeros_like(block)
    keys = (jnp.where(low, block, zero), jnp.where(low, zero, swapped))
    values = (jnp.where(low, swapped, zero), jnp.where(low, zero, block))
    return [k.astype(BF16) for k in keys], [v.astype(BF16) for v in values]


def attend(q, keys, values, allowed, sinks):
    total = None
    for h in range(2):
        scores = dot(q, keys[h], (1, 1)) * HEAD_DIM**-0.5
        scores = jnp.where(allowed, scores, -1e30)
        sink = sinks[h : h + 1, :1]
        peak = jnp.maximum(jnp.max(scores, axis=-1, keepdims=True), sink)
        terms = jnp.exp(scores - peak)
        total_terms = jnp.sum(terms, axis=-1, keepdims=True) + jnp.exp(sink - peak)
        probs = (terms / total_terms).astype(BF16)
        part = dot(probs, values[h])
        total = part if total is None else total + part
    return total.astype(BF16)


def project(attended, w_ref, out_ref, row0):
    for t in range(0, out_ref.shape[0], 2):
        both = dot(attended, w_ref[:, t * LANES : (t + 2) * LANES]).astype(BF16)
        out_ref[t, row0 : row0 + WINDOW, :] = both[:, :LANES]
        out_ref[t + 1, row0 : row0 + WINDOW, :] = both[:, LANES:]


def window_mask():
    row = lax.broadcasted_iota(jnp.int32, (WINDOW, 2 * WINDOW), 0)
    col = lax.broadcasted_iota(jnp.int32, (WINDOW, 2 * WINDOW), 1)
    return (col > row) & (col <= row + WINDOW), col


def fill_slots(cap, experts, routes_ref, weights_ref, send_ref, take_ref, cols_ref):
    tokens = routes_ref.shape[1]
    slots = send_ref.shape[0]
    expert_row = lax.broadcasted_iota(jnp.int32, (experts, tokens), 0)
    picks = [routes_ref[k : k + 1, :] for k in range(2)]
    hot = [(pick == expert_row).astype(F32) for pick in picks]
    r = lax.broadcasted_iota(jnp.int32, (tokens, tokens), 0)
    c = lax.broadcasted_iota(jnp.int32, (tokens, tokens), 1)
    ahead = dot((hot[0] + hot[1]).astype(BF16), (r < c).astype(BF16))
    targets = [picks[k].astype(F32) * cap + jnp.sum(ahead * hot[k], axis=0, keepdims=True) for k in range(2)]
    slot_row = lax.broadcasted_iota(jnp.int32, (slots, tokens), 0)
    here = [slot_row == target.astype(jnp.int32) for target in targets]
    send_ref[...] = (here[0] | here[1]).astype(F32).astype(BF16)
    row = lax.broadcasted_iota(jnp.int32, (8, tokens), 0)
    rows = [*targets, weights_ref[0:1, :], weights_ref[1:2, :]]
    table = jnp.zeros((8, tokens), F32)
    for i, values in enumerate(rows):
        table = jnp.where(row == i, values, table)
    cols = jnp.transpose(table)
    cols_ref[...] = cols
    slot_lane = lax.broadcasted_iota(jnp.int32, (tokens, slots), 1)
    for k in range(2):
        target = cols[:, k : k + 1].astype(jnp.int32)
        take_ref[k * tokens : (k + 1) * tokens, :] = (slot_lane == target).astype(F32).astype(BF16)


def later_body(cap, experts, sinks_ref, q_ref, kv_ref, w_ref, routes_ref, weights_ref, out_ref, send_ref, take_ref, cols_ref):
    keys, values = both_places(kv_ref[...].astype(F32))
    inside, _ = window_mask()
    project(attend(q_ref[WINDOW:, :], keys, values, inside, sinks_ref[...]), w_ref, out_ref, WINDOW)
    fill_slots(cap, experts, routes_ref, weights_ref, send_ref, take_ref, cols_ref)


def first_body(sinks_ref, q_ref, kv_ref, before_ref, w_ref, partial_ref, out_ref):
    keys, values = both_places(jnp.concatenate([before_ref[...], kv_ref[:WINDOW, :]], axis=0).astype(F32))
    inside, col = window_mask()
    allowed = inside & ((col >= WINDOW) | (lax.axis_index("sp") > 0))
    project(attend(q_ref[:WINDOW, :], keys, values, allowed, sinks_ref[...]), w_ref, out_ref, 0)


def later_and_slots(sinks, q, kv, w, routes, weights, experts, cap):
    tokens = q.shape[0]
    slots = experts * cap
    return pl.pallas_call(
        functools.partial(later_body, cap, experts),
        out_shape=(
            vmem_out((w.shape[1] // LANES, tokens, LANES)),
            vmem_out((slots, tokens)),
            vmem_out((2 * tokens, slots)),
            pltpu.VMEM((tokens, 8), F32),
        ),
        in_specs=[VMEM_SPEC] * 6,
        out_specs=(VMEM_SPEC,) * 4,
        compiler_params=small_kernel(16),
        cost_estimate=pl.CostEstimate(flops=10**9, bytes_accessed=2**20, transcendentals=2**16),
        name="later_and_slots",
    )(*in_vmem(sinks, q, kv, w, routes, weights))


def attention_first(sinks, q, kv, before, w, partial):
    shares = w.shape[1] // LANES
    return pl.pallas_call(
        first_body,
        out_shape=vmem_out(partial.shape),
        in_specs=[VMEM_SPEC] * 6,
        out_specs=VMEM_SPEC,
        input_output_aliases={5: 0},
        compiler_params=small_kernel(16),
        name="attention_first",
    )(*in_vmem(sinks, q, kv, before, w, partial))


def load_body(*refs):
    sources, (last_ref, kv_ref, sinks_ref, q_ref, w_ref, routes_ref, weights_ref, own_ref) = refs[:8], refs[8:16]
    k_ref, v_ref, sinks_smem, sems = refs[16:]
    k_hbm, v_hbm, q_hbm, w_hbm, sinks_hbm, routes_hbm, weights_hbm, stream_hbm = sources
    first_col = pl.multiple_of(lax.axis_index(TP) * LANES, LANES)
    pairs = (
        (k_hbm, k_ref),
        (v_hbm, v_ref),
        (q_hbm, q_ref),
        (w_hbm, w_ref),
        (sinks_hbm, sinks_smem),
        (routes_hbm, routes_ref),
        (weights_hbm, weights_ref),
        (stream_hbm.at[:, pl.ds(first_col, LANES)], own_ref),
    )
    copies = [pltpu.make_async_copy(source, target, sems.at[i]) for i, (source, target) in enumerate(pairs)]
    for copy in copies:
        copy.start()
    group = lax.axis_index(TP) * (q_ref.shape[1] // HEAD_DIM) // REP
    low = lax.broadcasted_iota(jnp.int32, kv_ref.shape, 1) < HEAD_DIM

    def head(ref):
        picked = ref[:, :LANES].astype(F32)
        for c in range(LANES, ref.shape[1], LANES):
            picked = jnp.where(group // 2 == c // LANES, ref[:, c : c + LANES].astype(F32), picked)
        return picked, jnp.concatenate([picked[:, HEAD_DIM:], picked[:, :HEAD_DIM]], axis=1)

    copies[0].wait()
    key, key_swapped = head(k_ref)
    copies[1].wait()
    value, value_swapped = head(v_ref)
    odd = group % 2 == 1
    kv = jnp.where(low, jnp.where(odd, key_swapped, key), jnp.where(odd, value, value_swapped)).astype(BF16)
    kv_ref[...] = kv
    last_ref[...] = kv[kv.shape[0] - WINDOW :]
    copies[4].wait()
    row = lax.broadcasted_iota(jnp.int32, sinks_ref.shape, 0)
    sinks_ref[...] = jnp.where(row == 0, sinks_smem[0], sinks_smem[1])
    for i in (2, 3, 5, 6, 7):
        copies[i].wait()


def loaded(k, v, q, w, sinks, routes, weights, stream_in):
    rows = q.shape[0]
    return pl.pallas_call(
        load_body,
        out_shape=(
            vmem_out((WINDOW, LANES)),
            vmem_out((rows, LANES)),
            pltpu.VMEM((8, LANES), F32),
            vmem_out(q.shape),
            vmem_out(w.shape),
            pltpu.VMEM(routes.shape, jnp.int32),
            pltpu.VMEM(weights.shape, F32),
            vmem_out((rows, LANES)),
        ),
        in_specs=[pl.BlockSpec(memory_space=pltpu.HBM)] * 8,
        out_specs=(VMEM_SPEC,) * 8,
        scratch_shapes=[
            pltpu.VMEM(k.shape, BF16),
            pltpu.VMEM(v.shape, BF16),
            pltpu.SMEM(sinks.shape, F32),
            pltpu.SemaphoreType.DMA((8,)),
        ],
        compiler_params=small_kernel(16),
        name="load",
    )(*in_hbm(k, v, q, w, sinks, routes, weights, stream_in))


def copies_body(rows_ref, out_ref):
    @pl.when(lax.axis_index("sp") % 2 == 1)
    def _():
        pl.delay(LAG_NS)

    rows = rows_ref[...]
    for t in range(out_ref.shape[0]):
        out_ref[t] = rows


def copied(rows, count):
    return pl.pallas_call(
        copies_body,
        out_shape=vmem_out((count, *rows.shape)),
        in_specs=[VMEM_SPEC],
        out_specs=VMEM_SPEC,
        compiler_params=small_kernel(16),
        name="copies",
    )(*in_vmem(rows))


def total_body(parts_ref, out_ref):
    rows = parts_ref.shape[1]
    block = 64
    for lo in range(0, rows, block):
        summed = parts_ref[0, lo : lo + block, :].astype(F32)
        for t in range(1, parts_ref.shape[0]):
            summed = summed + parts_ref[t, lo : lo + block, :].astype(F32)
        out_ref[lo : lo + block, :] = summed.astype(BF16)


def total(parts):
    return pl.pallas_call(
        total_body,
        out_shape=vmem_out(parts.shape[1:]),
        in_specs=[VMEM_SPEC],
        out_specs=VMEM_SPEC,
        compiler_params=small_kernel(16),
        name="total",
    )(*in_vmem(parts))


def stream_body(arrived_ref, own_ref, send_ref, stream_ref, rows_ref):
    summed = arrived_ref[0].astype(F32)
    for t in range(1, arrived_ref.shape[0]):
        summed = summed + arrived_ref[t].astype(F32)
    stream = (own_ref[...].astype(F32) + summed).astype(BF16)
    stream_ref[...] = stream
    rows_ref[...] = dot(send_ref[...], stream).astype(BF16)


def stream_and_rows(arrived, own, send):
    return pl.pallas_call(
        stream_body,
        out_shape=(vmem_out(own.shape), vmem_out((send.shape[0], LANES))),
        in_specs=[VMEM_SPEC] * 3,
        out_specs=(VMEM_SPEC, VMEM_SPEC),
        compiler_params=small_kernel(16),
        name="stream",
    )(*in_vmem(arrived, own, send))


def expert_body(block, x_ref, gain_ref, gate_ref, up_ref, down_ref, out_ref):
    shares, rows, _ = x_ref.shape
    for lo in range(0, rows, block):
        stream = jnp.concatenate([x_ref[t, lo : lo + block, :] for t in range(shares)], axis=1).astype(F32)
        scale = lax.rsqrt(jnp.mean(stream * stream, axis=-1, keepdims=True) + NORM_EPS)
        normed = (stream * scale * gain_ref[...]).astype(BF16)
        gate_act = dot(normed, gate_ref[0])
        up_act = dot(normed, up_ref[0])
        hidden = (gate_act * jax.nn.sigmoid(gate_act) * up_act).astype(BF16)
        for t in range(0, shares, 2):
            both = dot(hidden, down_ref[0, :, t * LANES : (t + 2) * LANES]).astype(BF16)
            out_ref[t, lo : lo + block, :] = both[:, :LANES]
            out_ref[t + 1, lo : lo + block, :] = both[:, LANES:]


def expert(x, gain, gate, up, down, block):
    return pl.pallas_call(
        functools.partial(expert_body, block),
        out_shape=vmem_out(x.shape),
        in_specs=[VMEM_SPEC] * 5,
        out_specs=VMEM_SPEC,
        cost_estimate=pl.CostEstimate(flops=6 * x.shape[1] * gate.shape[1] * gate.shape[2], bytes_accessed=2 * x.size * 2, transcendentals=0),
        compiler_params=small_kernel(24),
        name="expert",
    )(*in_vmem(x, gain, gate, up, down))


def combine_body(rows_ref, take_ref, weights_ref, stream_ref, out_ref):
    tokens = stream_ref.shape[0]
    taken = dot(take_ref[...], rows_ref[...])
    moe = taken[:tokens] * weights_ref[:, 2:3] + taken[tokens:] * weights_ref[:, 3:4]
    out_ref[...] = (stream_ref[...].astype(F32) + moe).astype(BF16)


def combine(rows, take, weights, stream):
    return pl.pallas_call(
        combine_body,
        out_shape=vmem_out(stream.shape),
        in_specs=[VMEM_SPEC] * 4,
        out_specs=VMEM_SPEC,
        compiler_params=small_kernel(16),
        name="combine",
    )(*in_vmem(rows, take, weights, stream))


def per_device(
    query_rows,
    key_rows,
    value_rows,
    sink_logits,
    out_weight,
    stream_in,
    norm_gain,
    routes,
    route_weights,
    gate_weight,
    up_weight,
    down_weight,
):
    tokens = query_rows.shape[0]
    tp_size = lax.axis_size(TP)
    experts = lax.axis_size("sp")
    cap = 3 * tokens * routes.shape[1] // (2 * experts)
    last, kv, sinks, queries, out_share, choices, weights, own = loaded(
        key_rows, value_rows, query_rows, out_weight, sink_logits, routes.T, route_weights.T, stream_in
    )
    before = lax.ppermute(last, "sp", [(i, i + 1) for i in range(experts - 1)])
    later, send, take, cols = later_and_slots(sinks, queries, kv, out_share, choices, weights, experts, cap)
    partial = attention_first(sinks, queries, kv, before, out_share, later)
    arrived = lax.all_to_all(partial, TP, split_axis=0, concat_axis=0, tiled=True)
    stream, rows = stream_and_rows(arrived, own, send)
    rows = lax.all_to_all(rows.reshape(experts, cap, LANES), "sp", split_axis=0, concat_axis=0, tiled=True)
    slots = experts * cap
    gain = norm_gain.reshape(1, -1)
    copies = copied(rows.reshape(slots, LANES), tp_size)
    features = lax.all_to_all(copies, TP, split_axis=0, concat_axis=0, tiled=True)
    parts = expert(features, gain, gate_weight, up_weight, down_weight, 384)
    summed = total(lax.all_to_all(parts, TP, split_axis=0, concat_axis=0, tiled=True))
    returned = lax.all_to_all(summed.reshape(experts, cap, LANES), "sp", split_axis=0, concat_axis=0, tiled=True)
    out = combine(returned.reshape(slots, LANES), take, cols, stream)
    return lax.all_to_all(out, TP, split_axis=0, concat_axis=1, tiled=True)


def solution(mesh):
    finer = Mesh(mesh.devices.reshape(mesh.shape["sp"], 4, 4), ("sp", "tp_0", "tp_1"))
    placed = (
        P("sp", TP),
        P("sp", None),
        P("sp", None),
        P(TP),
        P(TP, None),
        P("sp", None),
        P(),
        P("sp", None),
        P("sp", None),
        P("sp", None, TP),
        P("sp", None, TP),
        P("sp", TP, None),
    )
    return jax.shard_map(
        per_device, mesh=finer, in_specs=placed, out_specs=P(SP_TP, None), check_vma=False
    )
```

```python
import functools

import jax
import jax.numpy as jnp
from jax import lax
from jax.experimental import pallas as pl
from jax.experimental.pallas import tpu as pltpu
from jax.sharding import Mesh
from jax.sharding import PartitionSpec as P

HEAD_DIM = 64
REP = 8
WINDOW = 128
LANES = 128
TP = ("tp_0", "tp_1")
SP = ("z", "core")
PLANES = ("core", "tp_0", "tp_1")
SIDE = 4
NORM_EPS = 1e-06
BF16 = jnp.bfloat16
F32 = jnp.float32
VMEM_SPEC = pl.BlockSpec(memory_space=pltpu.VMEM)


def in_vmem(*arrays):
    return [pltpu.with_memory_space_constraint(a, pltpu.VMEM) for a in arrays]


def in_hbm(*arrays):
    return [pltpu.with_memory_space_constraint(a, pltpu.HBM) for a in arrays]


def small_kernel(mib):
    return pltpu.CompilerParams(vmem_limit_bytes=mib * 2**20)


def vmem_out(shape):
    return pltpu.VMEM(shape, BF16)


def dot(a, b, contract=(1, 0)):
    return lax.dot_general(a, b, (((contract[0],), (contract[1],)), ((), ())), preferred_element_type=F32)


def both_places(block):
    swapped = jnp.concatenate([block[:, HEAD_DIM:], block[:, :HEAD_DIM]], axis=1)
    low = lax.broadcasted_iota(jnp.int32, block.shape, 1) < HEAD_DIM
    zero = jnp.zeros_like(block)
    keys = (jnp.where(low, block, zero), jnp.where(low, zero, swapped))
    values = (jnp.where(low, swapped, zero), jnp.where(low, zero, block))
    return [k.astype(BF16) for k in keys], [v.astype(BF16) for v in values]


def attend(q, keys, values, allowed, sinks):
    total = None
    for h in range(2):
        scores = dot(q, keys[h], (1, 1)) * HEAD_DIM**-0.5
        scores = jnp.where(allowed, scores, -1e30)
        sink = sinks[h : h + 1, :1]
        peak = jnp.maximum(jnp.max(scores, axis=-1, keepdims=True), sink)
        terms = jnp.exp(scores - peak)
        total_terms = jnp.sum(terms, axis=-1, keepdims=True) + jnp.exp(sink - peak)
        probs = (terms / total_terms).astype(BF16)
        part = dot(probs, values[h])
        total = part if total is None else total + part
    return total.astype(BF16)


def project(attended, w_ref, out_ref, row0):
    for t in range(0, out_ref.shape[0], 2):
        both = dot(attended, w_ref[:, t * LANES : (t + 2) * LANES]).astype(BF16)
        out_ref[t, row0 : row0 + WINDOW, :] = both[:, :LANES]
        out_ref[t + 1, row0 : row0 + WINDOW, :] = both[:, LANES:]


def window_mask():
    row = lax.broadcasted_iota(jnp.int32, (WINDOW, 2 * WINDOW), 0)
    col = lax.broadcasted_iota(jnp.int32, (WINDOW, 2 * WINDOW), 1)
    return (col > row) & (col <= row + WINDOW), col


def fill_slots(cap, experts, routes_ref, weights_ref, send_ref, take_ref, cols_ref):
    tokens = routes_ref.shape[1]
    slots = send_ref.shape[0]
    expert_row = lax.broadcasted_iota(jnp.int32, (experts, tokens), 0)
    picks = [routes_ref[k : k + 1, :] for k in range(2)]
    hot = [(pick == expert_row).astype(F32) for pick in picks]
    r = lax.broadcasted_iota(jnp.int32, (tokens, tokens), 0)
    c = lax.broadcasted_iota(jnp.int32, (tokens, tokens), 1)
    ahead = dot((hot[0] + hot[1]).astype(BF16), (r < c).astype(BF16))
    targets = [picks[k].astype(F32) * cap + jnp.sum(ahead * hot[k], axis=0, keepdims=True) for k in range(2)]
    slot_row = lax.broadcasted_iota(jnp.int32, (slots, tokens), 0)
    here = [slot_row == target.astype(jnp.int32) for target in targets]
    send_ref[...] = (here[0] | here[1]).astype(F32).astype(BF16)
    row = lax.broadcasted_iota(jnp.int32, (8, tokens), 0)
    rows = [*targets, weights_ref[0:1, :], weights_ref[1:2, :]]
    table = jnp.zeros((8, tokens), F32)
    for i, values in enumerate(rows):
        table = jnp.where(row == i, values, table)
    cols = jnp.transpose(table)
    cols_ref[...] = cols
    slot_lane = lax.broadcasted_iota(jnp.int32, (tokens, slots), 1)
    for k in range(2):
        target = cols[:, k : k + 1].astype(jnp.int32)
        take_ref[k * tokens : (k + 1) * tokens, :] = (slot_lane == target).astype(F32).astype(BF16)


def later_body(cap, experts, sinks_ref, q_ref, kv_ref, w_ref, routes_ref, weights_ref, out_ref, send_ref, take_ref, cols_ref):
    keys, values = both_places(kv_ref[...].astype(F32))
    inside, _ = window_mask()
    project(attend(q_ref[WINDOW:, :], keys, values, inside, sinks_ref[...]), w_ref, out_ref, WINDOW)
    fill_slots(cap, experts, routes_ref, weights_ref, send_ref, take_ref, cols_ref)


def first_body(sinks_ref, q_ref, kv_ref, before_ref, w_ref, partial_ref, out_ref):
    keys, values = both_places(jnp.concatenate([before_ref[...], kv_ref[:WINDOW, :]], axis=0).astype(F32))
    inside, col = window_mask()
    allowed = inside & ((col >= WINDOW) | (lax.axis_index(SP) > 0))
    project(attend(q_ref[:WINDOW, :], keys, values, allowed, sinks_ref[...]), w_ref, out_ref, 0)


def later_and_slots(sinks, q, kv, w, routes, weights, experts, cap):
    tokens = q.shape[0]
    slots = experts * cap
    return pl.pallas_call(
        functools.partial(later_body, cap, experts),
        out_shape=(
            vmem_out((w.shape[1] // LANES, tokens, LANES)),
            vmem_out((slots, tokens)),
            vmem_out((2 * tokens, slots)),
            pltpu.VMEM((tokens, 8), F32),
        ),
        in_specs=[VMEM_SPEC] * 6,
        out_specs=(VMEM_SPEC,) * 4,
        compiler_params=small_kernel(16),
        cost_estimate=pl.CostEstimate(flops=10**9, bytes_accessed=2**20, transcendentals=2**16),
        name="later_and_slots",
    )(*in_vmem(sinks, q, kv, w, routes, weights))


def attention_first(sinks, q, kv, before, w, partial):
    shares = w.shape[1] // LANES
    return pl.pallas_call(
        first_body,
        out_shape=vmem_out(partial.shape),
        in_specs=[VMEM_SPEC] * 6,
        out_specs=VMEM_SPEC,
        input_output_aliases={5: 0},
        compiler_params=small_kernel(16),
        name="attention_first",
    )(*in_vmem(sinks, q, kv, before, w, partial))


def load_body(*refs):
    sources, (last_ref, kv_ref, sinks_ref, q_ref, w_ref, routes_ref, weights_ref, own_ref) = refs[:8], refs[8:16]
    k_ref, v_ref, sinks_smem, sems = refs[16:]
    k_hbm, v_hbm, q_hbm, w_hbm, sinks_hbm, routes_hbm, weights_hbm, stream_hbm = sources
    first_col = pl.multiple_of(lax.axis_index(TP) * LANES, LANES)
    pairs = (
        (k_hbm, k_ref),
        (v_hbm, v_ref),
        (q_hbm, q_ref),
        (w_hbm, w_ref),
        (sinks_hbm, sinks_smem),
        (routes_hbm, routes_ref),
        (weights_hbm, weights_ref),
        (stream_hbm.at[:, pl.ds(first_col, LANES)], own_ref),
    )
    copies = [pltpu.make_async_copy(source, target, sems.at[i]) for i, (source, target) in enumerate(pairs)]
    for copy in copies:
        copy.start()
    group = lax.axis_index(TP) * (q_ref.shape[1] // HEAD_DIM) // REP
    low = lax.broadcasted_iota(jnp.int32, kv_ref.shape, 1) < HEAD_DIM

    def head(ref):
        picked = ref[:, :LANES].astype(F32)
        for c in range(LANES, ref.shape[1], LANES):
            picked = jnp.where(group // 2 == c // LANES, ref[:, c : c + LANES].astype(F32), picked)
        return picked, jnp.concatenate([picked[:, HEAD_DIM:], picked[:, :HEAD_DIM]], axis=1)

    copies[0].wait()
    key, key_swapped = head(k_ref)
    copies[1].wait()
    value, value_swapped = head(v_ref)
    odd = group % 2 == 1
    kv = jnp.where(low, jnp.where(odd, key_swapped, key), jnp.where(odd, value, value_swapped)).astype(BF16)
    kv_ref[...] = kv
    last_ref[...] = kv[kv.shape[0] - WINDOW :]
    copies[4].wait()
    row = lax.broadcasted_iota(jnp.int32, sinks_ref.shape, 0)
    sinks_ref[...] = jnp.where(row == 0, sinks_smem[0], sinks_smem[1])
    for i in (2, 3, 5, 6, 7):
        copies[i].wait()


def loaded(k, v, q, w, sinks, routes, weights, stream_in):
    rows = q.shape[0]
    return pl.pallas_call(
        load_body,
        out_shape=(
            vmem_out((WINDOW, LANES)),
            vmem_out((rows, LANES)),
            pltpu.VMEM((8, LANES), F32),
            vmem_out(q.shape),
            vmem_out(w.shape),
            pltpu.VMEM(routes.shape, jnp.int32),
            pltpu.VMEM(weights.shape, F32),
            vmem_out((rows, LANES)),
        ),
        in_specs=[pl.BlockSpec(memory_space=pltpu.HBM)] * 8,
        out_specs=(VMEM_SPEC,) * 8,
        scratch_shapes=[
            pltpu.VMEM(k.shape, BF16),
            pltpu.VMEM(v.shape, BF16),
            pltpu.SMEM(sinks.shape, F32),
            pltpu.SemaphoreType.DMA((8,)),
        ],
        compiler_params=small_kernel(16),
        name="load",
    )(*in_hbm(k, v, q, w, sinks, routes, weights, stream_in))


def copies_body(rows_ref, out_ref):
    rows = rows_ref[...]
    for t in range(out_ref.shape[0]):
        out_ref[t] = rows


def copied(rows, count):
    return pl.pallas_call(
        copies_body,
        out_shape=vmem_out((count, *rows.shape)),
        in_specs=[VMEM_SPEC],
        out_specs=VMEM_SPEC,
        compiler_params=small_kernel(16),
        name="copies",
    )(*in_vmem(rows))


def total_body(parts_ref, out_ref):
    rows = parts_ref.shape[1]
    block = 128
    for lo in range(0, rows, block):
        summed = parts_ref[0, lo : lo + block, :].astype(F32)
        for t in range(1, parts_ref.shape[0]):
            summed = summed + parts_ref[t, lo : lo + block, :].astype(F32)
        out_ref[lo : lo + block, :] = summed.astype(BF16)


def total(parts):
    return pl.pallas_call(
        total_body,
        out_shape=vmem_out(parts.shape[1:]),
        in_specs=[VMEM_SPEC],
        out_specs=VMEM_SPEC,
        compiler_params=small_kernel(16),
        name="total",
    )(*in_vmem(parts))


def stream_body(arrived_ref, own_ref, send_ref, stream_ref, rows_ref):
    summed = arrived_ref[0].astype(F32)
    for t in range(1, arrived_ref.shape[0]):
        summed = summed + arrived_ref[t].astype(F32)
    stream = (own_ref[...].astype(F32) + summed).astype(BF16)
    stream_ref[...] = stream
    rows_ref[...] = dot(send_ref[...], stream).astype(BF16)


def stream_and_rows(arrived, own, send):
    return pl.pallas_call(
        stream_body,
        out_shape=(vmem_out(own.shape), vmem_out((send.shape[0], LANES))),
        in_specs=[VMEM_SPEC] * 3,
        out_specs=(VMEM_SPEC, VMEM_SPEC),
        compiler_params=small_kernel(16),
        name="stream",
    )(*in_vmem(arrived, own, send))


def expert_body(block, x_ref, gain_ref, gate_ref, up_ref, down_ref, out_ref):
    shares, rows, _ = x_ref.shape
    flipped = lax.axis_index("core") == 1
    place = [jnp.where(flipped, t % SIDE * SIDE + t // SIDE, t) for t in range(shares)]
    for lo in range(0, rows, block):
        stream = jnp.concatenate([x_ref[place[t], lo : lo + block, :] for t in range(shares)], axis=1).astype(F32)
        scaled = (stream * gain_ref[...]).astype(BF16)
        scale = lax.rsqrt(jnp.mean(stream * stream, axis=-1, keepdims=True) + NORM_EPS)
        gate_act = dot(scaled, gate_ref[0]) * scale
        up_act = dot(scaled, up_ref[0]) * scale
        hidden = (gate_act * jax.nn.sigmoid(gate_act) * up_act).astype(BF16)
        for t in range(0, shares, 2):
            both = dot(hidden, down_ref[0, :, t * LANES : (t + 2) * LANES]).astype(BF16)
            out_ref[place[t], lo : lo + block, :] = both[:, :LANES]
            out_ref[place[t + 1], lo : lo + block, :] = both[:, LANES:]


def expert(x, gain, gate, up, down, block):
    return pl.pallas_call(
        functools.partial(expert_body, block),
        out_shape=vmem_out(x.shape),
        in_specs=[VMEM_SPEC] * 5,
        out_specs=VMEM_SPEC,
        cost_estimate=pl.CostEstimate(flops=6 * x.shape[1] * gate.shape[1] * gate.shape[2], bytes_accessed=2 * x.size * 2, transcendentals=0),
        compiler_params=small_kernel(24),
        name="expert",
    )(*in_vmem(x, gain, gate, up, down))


def combine_body(rows_ref, take_ref, weights_ref, stream_ref, out_ref):
    tokens = stream_ref.shape[0]
    taken = dot(take_ref[...], rows_ref[...])
    moe = taken[:tokens] * weights_ref[:, 2:3] + taken[tokens:] * weights_ref[:, 3:4]
    out_ref[...] = (stream_ref[...].astype(F32) + moe).astype(BF16)


def combine(rows, take, weights, stream):
    return pl.pallas_call(
        combine_body,
        out_shape=vmem_out(stream.shape),
        in_specs=[VMEM_SPEC] * 4,
        out_specs=VMEM_SPEC,
        compiler_params=small_kernel(16),
        name="combine",
    )(*in_vmem(rows, take, weights, stream))


def lines(core, dim):
    at = [[core * SIDE * SIDE + y * SIDE + x for x in range(SIDE)] for y in range(SIDE)]
    return at if dim == 1 else [list(line) for line in zip(*at)]


LINES = lines(0, 1) + lines(1, 0)
CROSSING = lines(0, 0) + lines(1, 1)


def along(parts, groups):
    return lax.all_to_all(parts, PLANES, split_axis=0, concat_axis=0, axis_index_groups=groups, tiled=True)


def per_device(
    query_rows,
    key_rows,
    value_rows,
    sink_logits,
    out_weight,
    stream_in,
    norm_gain,
    routes,
    route_weights,
    gate_weight,
    up_weight,
    down_weight,
):
    tokens = query_rows.shape[0]
    tp_size = lax.axis_size(TP)
    experts = lax.axis_size(SP)
    cap = 3 * tokens * routes.shape[1] // (2 * experts)
    last, kv, sinks, queries, out_share, choices, weights, own = loaded(
        key_rows, value_rows, query_rows, out_weight, sink_logits, routes.T, route_weights.T, stream_in
    )
    before = lax.ppermute(last, SP, [(i, i + 1) for i in range(experts - 1)])
    later, send, take, cols = later_and_slots(sinks, queries, kv, out_share, choices, weights, experts, cap)
    partial = attention_first(sinks, queries, kv, before, out_share, later)
    arrived = lax.all_to_all(partial, TP, split_axis=0, concat_axis=0, tiled=True)
    stream, rows = stream_and_rows(arrived, own, send)
    rows = lax.all_to_all(rows.reshape(experts, cap, LANES), SP, split_axis=0, concat_axis=0, tiled=True)
    slots = experts * cap
    gain = norm_gain.reshape(1, -1)
    features = rows.reshape(slots, LANES)
    for groups in (LINES, CROSSING):
        features = along(copied(features, SIDE), groups).reshape(-1, LANES)
    parts = expert(features.reshape(tp_size, slots, LANES), gain, gate_weight, up_weight, down_weight, 384)
    for groups in (CROSSING, LINES):
        parts = total(along(parts.reshape(SIDE, -1, LANES), groups))
    summed = parts
    returned = lax.all_to_all(summed.reshape(experts, cap, LANES), SP, split_axis=0, concat_axis=0, tiled=True)
    out = combine(returned.reshape(slots, LANES), take, cols, stream)
    return lax.all_to_all(out, TP, split_axis=0, concat_axis=1, tiled=True)


def solution(mesh):
    finer = Mesh(mesh.devices.reshape(-1, 2, SIDE, SIDE), (*SP, *TP))
    placed = (
        P(SP, TP),
        P(SP, None),
        P(SP, None),
        P(TP),
        P(TP, None),
        P(SP, None),
        P(),
        P(SP, None),
        P(SP, None),
        P(SP, None, TP),
        P(SP, None, TP),
        P(SP, TP, None),
    )
    return jax.shard_map(
        per_device, mesh=finer, in_specs=placed, out_specs=P((*SP, *TP), None), check_vma=False
    )
```

```python
import functools

import jax
import jax.numpy as jnp
from jax import lax
from jax.experimental import pallas as pl
from jax.experimental.pallas import tpu as pltpu
from jax.sharding import Mesh
from jax.sharding import PartitionSpec as P

HEAD_DIM = 64
REP = 8
WINDOW = 128
LANES = 128
TP = ("tp_0", "tp_1")
SP = ("z", "core")
PLANES = ("core", "tp_0", "tp_1")
SIDE = 4
NORM_EPS = 1e-06
BF16 = jnp.bfloat16
F32 = jnp.float32
VMEM_SPEC = pl.BlockSpec(memory_space=pltpu.VMEM)


def in_vmem(*arrays):
    return [pltpu.with_memory_space_constraint(a, pltpu.VMEM) for a in arrays]


def in_hbm(*arrays):
    return [pltpu.with_memory_space_constraint(a, pltpu.HBM) for a in arrays]


def small_kernel(mib):
    return pltpu.CompilerParams(vmem_limit_bytes=mib * 2**20)


def vmem_out(shape):
    return pltpu.VMEM(shape, BF16)


def dot(a, b, contract=(1, 0)):
    return lax.dot_general(a, b, (((contract[0],), (contract[1],)), ((), ())), preferred_element_type=F32)


def both_places(block):
    swapped = jnp.concatenate([block[:, HEAD_DIM:], block[:, :HEAD_DIM]], axis=1)
    low = lax.broadcasted_iota(jnp.int32, block.shape, 1) < HEAD_DIM
    zero = jnp.zeros_like(block)
    keys = (jnp.where(low, block, zero), jnp.where(low, zero, swapped))
    values = (jnp.where(low, swapped, zero), jnp.where(low, zero, block))
    return [k.astype(BF16) for k in keys], [v.astype(BF16) for v in values]


def attend(q, keys, values, allowed, sinks):
    total = None
    for h in range(2):
        scores = dot(q, keys[h], (1, 1)) * HEAD_DIM**-0.5
        scores = jnp.where(allowed, scores, -1e30)
        sink = sinks[h : h + 1, :1]
        peak = jnp.maximum(jnp.max(scores, axis=-1, keepdims=True), sink)
        terms = jnp.exp(scores - peak)
        total_terms = jnp.sum(terms, axis=-1, keepdims=True) + jnp.exp(sink - peak)
        probs = (terms / total_terms).astype(BF16)
        part = dot(probs, values[h])
        total = part if total is None else total + part
    return total.astype(BF16)


def project(attended, w_ref, out_ref, row0):
    for t in range(0, out_ref.shape[0], 2):
        both = dot(attended, w_ref[:, t * LANES : (t + 2) * LANES]).astype(BF16)
        out_ref[t, row0 : row0 + WINDOW, :] = both[:, :LANES]
        out_ref[t + 1, row0 : row0 + WINDOW, :] = both[:, LANES:]


def window_mask():
    row = lax.broadcasted_iota(jnp.int32, (WINDOW, 2 * WINDOW), 0)
    col = lax.broadcasted_iota(jnp.int32, (WINDOW, 2 * WINDOW), 1)
    return (col > row) & (col <= row + WINDOW), col


def fill_slots(cap, experts, routes_ref, weights_ref, send_ref, take_ref, cols_ref):
    tokens = routes_ref.shape[1]
    slots = send_ref.shape[0]
    expert_row = lax.broadcasted_iota(jnp.int32, (experts, tokens), 0)
    picks = [routes_ref[k : k + 1, :] for k in range(2)]
    hot = [(pick == expert_row).astype(F32) for pick in picks]
    r = lax.broadcasted_iota(jnp.int32, (tokens, tokens), 0)
    c = lax.broadcasted_iota(jnp.int32, (tokens, tokens), 1)
    ahead = dot((hot[0] + hot[1]).astype(BF16), (r < c).astype(BF16))
    targets = [picks[k].astype(F32) * cap + jnp.sum(ahead * hot[k], axis=0, keepdims=True) for k in range(2)]
    slot_row = lax.broadcasted_iota(jnp.int32, (slots, tokens), 0)
    here = [slot_row == target.astype(jnp.int32) for target in targets]
    send_ref[...] = (here[0] | here[1]).astype(F32).astype(BF16)
    row = lax.broadcasted_iota(jnp.int32, (8, tokens), 0)
    rows = [*targets, weights_ref[0:1, :], weights_ref[1:2, :]]
    table = jnp.zeros((8, tokens), F32)
    for i, values in enumerate(rows):
        table = jnp.where(row == i, values, table)
    cols = jnp.transpose(table)
    cols_ref[...] = cols
    slot_lane = lax.broadcasted_iota(jnp.int32, (tokens, slots), 1)
    for k in range(2):
        target = cols[:, k : k + 1].astype(jnp.int32)
        take_ref[k * tokens : (k + 1) * tokens, :] = (slot_lane == target).astype(F32).astype(BF16)


def later_body(cap, experts, sinks_ref, q_ref, kv_ref, w_ref, routes_ref, weights_ref, out_ref, send_ref, take_ref, cols_ref):
    keys, values = both_places(kv_ref[...].astype(F32))
    inside, _ = window_mask()
    project(attend(q_ref[WINDOW:, :], keys, values, inside, sinks_ref[...]), w_ref, out_ref, WINDOW)
    fill_slots(cap, experts, routes_ref, weights_ref, send_ref, take_ref, cols_ref)


def first_body(sinks_ref, q_ref, kv_ref, before_ref, w_ref, partial_ref, out_ref):
    keys, values = both_places(jnp.concatenate([before_ref[...], kv_ref[:WINDOW, :]], axis=0).astype(F32))
    inside, col = window_mask()
    allowed = inside & ((col >= WINDOW) | (lax.axis_index(SP) > 0))
    project(attend(q_ref[:WINDOW, :], keys, values, allowed, sinks_ref[...]), w_ref, out_ref, 0)


def later_and_slots(sinks, q, kv, w, routes, weights, experts, cap):
    tokens = q.shape[0]
    slots = experts * cap
    return pl.pallas_call(
        functools.partial(later_body, cap, experts),
        out_shape=(
            vmem_out((w.shape[1] // LANES, tokens, LANES)),
            vmem_out((slots, tokens)),
            vmem_out((2 * tokens, slots)),
            pltpu.VMEM((tokens, 8), F32),
        ),
        in_specs=[VMEM_SPEC] * 6,
        out_specs=(VMEM_SPEC,) * 4,
        compiler_params=small_kernel(16),
        cost_estimate=pl.CostEstimate(flops=10**9, bytes_accessed=2**20, transcendentals=2**16),
        name="later_and_slots",
    )(*in_vmem(sinks, q, kv, w, routes, weights))


def attention_first(sinks, q, kv, before, w, partial):
    shares = w.shape[1] // LANES
    return pl.pallas_call(
        first_body,
        out_shape=vmem_out(partial.shape),
        in_specs=[VMEM_SPEC] * 6,
        out_specs=VMEM_SPEC,
        input_output_aliases={5: 0},
        compiler_params=small_kernel(16),
        name="attention_first",
    )(*in_vmem(sinks, q, kv, before, w, partial))


def load_body(*refs):
    sources, (last_ref, kv_ref, sinks_ref, q_ref, w_ref, routes_ref, weights_ref, own_ref) = refs[:8], refs[8:16]
    k_ref, v_ref, sinks_smem, sems = refs[16:]
    k_hbm, v_hbm, q_hbm, w_hbm, sinks_hbm, routes_hbm, weights_hbm, stream_hbm = sources
    first_col = pl.multiple_of(lax.axis_index(TP) * LANES, LANES)
    pairs = (
        (k_hbm, k_ref),
        (v_hbm, v_ref),
        (q_hbm, q_ref),
        (w_hbm, w_ref),
        (sinks_hbm, sinks_smem),
        (routes_hbm, routes_ref),
        (weights_hbm, weights_ref),
        (stream_hbm.at[:, pl.ds(first_col, LANES)], own_ref),
    )
    copies = [pltpu.make_async_copy(source, target, sems.at[i]) for i, (source, target) in enumerate(pairs)]
    for copy in copies:
        copy.start()
    group = lax.axis_index(TP) * (q_ref.shape[1] // HEAD_DIM) // REP
    low = lax.broadcasted_iota(jnp.int32, kv_ref.shape, 1) < HEAD_DIM

    def head(ref):
        picked = ref[:, :LANES].astype(F32)
        for c in range(LANES, ref.shape[1], LANES):
            picked = jnp.where(group // 2 == c // LANES, ref[:, c : c + LANES].astype(F32), picked)
        return picked, jnp.concatenate([picked[:, HEAD_DIM:], picked[:, :HEAD_DIM]], axis=1)

    copies[0].wait()
    key, key_swapped = head(k_ref)
    copies[1].wait()
    value, value_swapped = head(v_ref)
    odd = group % 2 == 1
    kv = jnp.where(low, jnp.where(odd, key_swapped, key), jnp.where(odd, value, value_swapped)).astype(BF16)
    kv_ref[...] = kv
    last_ref[...] = kv[kv.shape[0] - WINDOW :]
    copies[4].wait()
    row = lax.broadcasted_iota(jnp.int32, sinks_ref.shape, 0)
    sinks_ref[...] = jnp.where(row == 0, sinks_smem[0], sinks_smem[1])
    for i in (2, 3, 5, 6, 7):
        copies[i].wait()


def loaded(k, v, q, w, sinks, routes, weights, stream_in):
    rows = q.shape[0]
    return pl.pallas_call(
        load_body,
        out_shape=(
            vmem_out((WINDOW, LANES)),
            vmem_out((rows, LANES)),
            pltpu.VMEM((8, LANES), F32),
            vmem_out(q.shape),
            vmem_out(w.shape),
            pltpu.VMEM(routes.shape, jnp.int32),
            pltpu.VMEM(weights.shape, F32),
            vmem_out((rows, LANES)),
        ),
        in_specs=[pl.BlockSpec(memory_space=pltpu.HBM)] * 8,
        out_specs=(VMEM_SPEC,) * 8,
        scratch_shapes=[
            pltpu.VMEM(k.shape, BF16),
            pltpu.VMEM(v.shape, BF16),
            pltpu.SMEM(sinks.shape, F32),
            pltpu.SemaphoreType.DMA((8,)),
        ],
        compiler_params=small_kernel(16),
        name="load",
    )(*in_hbm(k, v, q, w, sinks, routes, weights, stream_in))


def copies_body(rows_ref, out_ref):
    rows = rows_ref[...]
    for t in range(out_ref.shape[0]):
        out_ref[t] = rows


def copied(rows, count):
    return pl.pallas_call(
        copies_body,
        out_shape=vmem_out((count, *rows.shape)),
        in_specs=[VMEM_SPEC],
        out_specs=VMEM_SPEC,
        compiler_params=small_kernel(16),
        name="copies",
    )(*in_vmem(rows))


def total_body(parts_ref, out_ref):
    rows = parts_ref.shape[1]
    block = 128
    for lo in range(0, rows, block):
        summed = parts_ref[0, lo : lo + block, :].astype(F32)
        for t in range(1, parts_ref.shape[0]):
            summed = summed + parts_ref[t, lo : lo + block, :].astype(F32)
        out_ref[lo : lo + block, :] = summed.astype(BF16)


def total(parts):
    return pl.pallas_call(
        total_body,
        out_shape=vmem_out(parts.shape[1:]),
        in_specs=[VMEM_SPEC],
        out_specs=VMEM_SPEC,
        compiler_params=small_kernel(16),
        name="total",
    )(*in_vmem(parts))


def stream_body(arrived_ref, own_ref, send_ref, stream_ref, rows_ref):
    summed = arrived_ref[0].astype(F32)
    for t in range(1, arrived_ref.shape[0]):
        summed = summed + arrived_ref[t].astype(F32)
    stream = (own_ref[...].astype(F32) + summed).astype(BF16)
    stream_ref[...] = stream
    rows_ref[...] = dot(send_ref[...], stream).astype(BF16)


def stream_and_rows(arrived, own, send):
    return pl.pallas_call(
        stream_body,
        out_shape=(vmem_out(own.shape), vmem_out((send.shape[0], LANES))),
        in_specs=[VMEM_SPEC] * 3,
        out_specs=(VMEM_SPEC, VMEM_SPEC),
        compiler_params=small_kernel(16),
        name="stream",
    )(*in_vmem(arrived, own, send))


def expert_body(block, x_ref, gain_ref, gate_ref, up_ref, down_ref, out_ref):
    shares, rows, _ = x_ref.shape
    flipped = lax.axis_index("core") == 1
    place = [jnp.where(flipped, t % SIDE * SIDE + t // SIDE, t) for t in range(shares)]
    for lo in range(0, rows, block):
        stream = jnp.concatenate([x_ref[place[t], lo : lo + block, :] for t in range(shares)], axis=1).astype(F32)
        scaled = (stream * gain_ref[...]).astype(BF16)
        scale = lax.rsqrt(jnp.mean(stream * stream, axis=-1, keepdims=True) + NORM_EPS)
        gate_act = dot(scaled, gate_ref[0]) * scale
        up_act = dot(scaled, up_ref[0]) * scale
        hidden = (gate_act * jax.nn.sigmoid(gate_act) * up_act).astype(BF16)
        for t in range(0, shares, 2):
            both = dot(hidden, down_ref[0, :, t * LANES : (t + 2) * LANES]).astype(BF16)
            out_ref[place[t], lo : lo + block, :] = both[:, :LANES]
            out_ref[place[t + 1], lo : lo + block, :] = both[:, LANES:]


def expert(x, gain, gate, up, down, block):
    return pl.pallas_call(
        functools.partial(expert_body, block),
        out_shape=vmem_out(x.shape),
        in_specs=[VMEM_SPEC] * 5,
        out_specs=VMEM_SPEC,
        cost_estimate=pl.CostEstimate(flops=6 * x.shape[1] * gate.shape[1] * gate.shape[2], bytes_accessed=2 * x.size * 2, transcendentals=0),
        compiler_params=small_kernel(24),
        name="expert",
    )(*in_vmem(x, gain, gate, up, down))


def combine_body(rows_ref, take_ref, weights_ref, stream_ref, out_ref):
    tokens = stream_ref.shape[0]
    taken = dot(take_ref[...], rows_ref[...])
    moe = taken[:tokens] * weights_ref[:, 2:3] + taken[tokens:] * weights_ref[:, 3:4]
    out_ref[...] = (stream_ref[...].astype(F32) + moe).astype(BF16)


def combine(rows, take, weights, stream):
    return pl.pallas_call(
        combine_body,
        out_shape=vmem_out(stream.shape),
        in_specs=[VMEM_SPEC] * 4,
        out_specs=VMEM_SPEC,
        compiler_params=small_kernel(16),
        name="combine",
    )(*in_vmem(rows, take, weights, stream))


def lines(core, dim):
    at = [[core * SIDE * SIDE + y * SIDE + x for x in range(SIDE)] for y in range(SIDE)]
    return at if dim == 1 else [list(line) for line in zip(*at)]


LINES = lines(0, 1) + lines(1, 0)
CROSSING = lines(0, 0) + lines(1, 1)


def along(parts, groups):
    return lax.all_to_all(parts, PLANES, split_axis=0, concat_axis=0, axis_index_groups=groups, tiled=True)


def per_device(
    query_rows,
    key_rows,
    value_rows,
    sink_logits,
    out_weight,
    stream_in,
    norm_gain,
    routes,
    route_weights,
    gate_weight,
    up_weight,
    down_weight,
):
    tokens = query_rows.shape[0]
    tp_size = lax.axis_size(TP)
    experts = lax.axis_size(SP)
    cap = 3 * tokens * routes.shape[1] // (2 * experts)
    last, kv, sinks, queries, out_share, choices, weights, own = loaded(
        key_rows, value_rows, query_rows, out_weight, sink_logits, routes.T, route_weights.T, stream_in
    )
    before = lax.ppermute(last, SP, [(i, i + 1) for i in range(experts - 1)])
    later, send, take, cols = later_and_slots(sinks, queries, kv, out_share, choices, weights, experts, cap)
    partial = attention_first(sinks, queries, kv, before, out_share, later)
    arrived = lax.all_to_all(partial, TP, split_axis=0, concat_axis=0, tiled=True)
    stream, rows = stream_and_rows(arrived, own, send)
    rows = lax.all_to_all(rows.reshape(experts, cap, LANES), SP, split_axis=0, concat_axis=0, tiled=True)
    slots = experts * cap
    gain = norm_gain.reshape(1, -1)
    features = rows.reshape(slots, LANES)
    for groups in (LINES, CROSSING):
        features = along(copied(features, SIDE), groups).reshape(-1, LANES)
    parts = expert(features.reshape(tp_size, slots, LANES), gain, gate_weight, up_weight, down_weight, slots)
    for groups in (CROSSING, LINES):
        parts = total(along(parts.reshape(SIDE, -1, LANES), groups))
    summed = parts
    returned = lax.all_to_all(summed.reshape(experts, cap, LANES), SP, split_axis=0, concat_axis=0, tiled=True)
    out = combine(returned.reshape(slots, LANES), take, cols, stream)
    return lax.all_to_all(out, TP, split_axis=0, concat_axis=1, tiled=True)


def solution(mesh):
    finer = Mesh(mesh.devices.reshape(-1, 2, SIDE, SIDE), (*SP, *TP))
    placed = (
        P(SP, TP),
        P(SP, None),
        P(SP, None),
        P(TP),
        P(TP, None),
        P(SP, None),
        P(),
        P(SP, None),
        P(SP, None),
        P(SP, None, TP),
        P(SP, None, TP),
        P(SP, TP, None),
    )
    return jax.shard_map(
        per_device, mesh=finer, in_specs=placed, out_specs=P((*SP, *TP), None), check_vma=False
    )
```

```python
import functools

import jax
import jax.numpy as jnp
from jax import lax
from jax.experimental import pallas as pl
from jax.experimental.pallas import tpu as pltpu
from jax.sharding import Mesh
from jax.sharding import PartitionSpec as P

HEAD_DIM = 64
REP = 8
WINDOW = 128
LANES = 128
TP = ("tp_0", "tp_1")
SP = ("z", "core")
PLANES = ("core", "tp_0", "tp_1")
SIDE = 4
NORM_EPS = 1e-06
BF16 = jnp.bfloat16
F32 = jnp.float32
VMEM_SPEC = pl.BlockSpec(memory_space=pltpu.VMEM)


def in_vmem(*arrays):
    return [pltpu.with_memory_space_constraint(a, pltpu.VMEM) for a in arrays]


def in_hbm(*arrays):
    return [pltpu.with_memory_space_constraint(a, pltpu.HBM) for a in arrays]


def small_kernel(mib):
    return pltpu.CompilerParams(vmem_limit_bytes=mib * 2**20)


def vmem_out(shape):
    return pltpu.VMEM(shape, BF16)


def dot(a, b, contract=(1, 0)):
    return lax.dot_general(a, b, (((contract[0],), (contract[1],)), ((), ())), preferred_element_type=F32)


def both_places(block):
    swapped = jnp.concatenate([block[:, HEAD_DIM:], block[:, :HEAD_DIM]], axis=1)
    low = lax.broadcasted_iota(jnp.int32, block.shape, 1) < HEAD_DIM
    zero = jnp.zeros_like(block)
    keys = (jnp.where(low, block, zero), jnp.where(low, zero, swapped))
    values = (jnp.where(low, swapped, zero), jnp.where(low, zero, block))
    return [k.astype(BF16) for k in keys], [v.astype(BF16) for v in values]


def attend(q, keys, values, allowed, sinks):
    total = None
    for h in range(2):
        scores = dot(q, keys[h], (1, 1)) * HEAD_DIM**-0.5
        scores = jnp.where(allowed, scores, -1e30)
        sink = sinks[h : h + 1, :1]
        peak = jnp.maximum(jnp.max(scores, axis=-1, keepdims=True), sink)
        terms = jnp.exp(scores - peak)
        total_terms = jnp.sum(terms, axis=-1, keepdims=True) + jnp.exp(sink - peak)
        probs = (terms / total_terms).astype(BF16)
        part = dot(probs, values[h])
        total = part if total is None else total + part
    return total.astype(BF16)


def project(attended, w_ref, out_ref, row0):
    for t in range(0, out_ref.shape[0], 2):
        both = dot(attended, w_ref[:, t * LANES : (t + 2) * LANES]).astype(BF16)
        out_ref[t, row0 : row0 + WINDOW, :] = both[:, :LANES]
        out_ref[t + 1, row0 : row0 + WINDOW, :] = both[:, LANES:]


def window_mask():
    row = lax.broadcasted_iota(jnp.int32, (WINDOW, 2 * WINDOW), 0)
    col = lax.broadcasted_iota(jnp.int32, (WINDOW, 2 * WINDOW), 1)
    return (col > row) & (col <= row + WINDOW), col


def fill_slots(cap, experts, routes_ref, weights_ref, send_ref, take_ref, cols_ref):
    tokens = routes_ref.shape[1]
    slots = send_ref.shape[0]
    expert_row = lax.broadcasted_iota(jnp.int32, (experts, tokens), 0)
    picks = [routes_ref[k : k + 1, :] for k in range(2)]
    hot = [(pick == expert_row).astype(F32) for pick in picks]
    r = lax.broadcasted_iota(jnp.int32, (tokens, tokens), 0)
    c = lax.broadcasted_iota(jnp.int32, (tokens, tokens), 1)
    ahead = dot((hot[0] + hot[1]).astype(BF16), (r < c).astype(BF16))
    targets = [picks[k].astype(F32) * cap + jnp.sum(ahead * hot[k], axis=0, keepdims=True) for k in range(2)]
    slot_row = lax.broadcasted_iota(jnp.int32, (slots, tokens), 0)
    here = [slot_row == target.astype(jnp.int32) for target in targets]
    send_ref[...] = (here[0] | here[1]).astype(F32).astype(BF16)
    row = lax.broadcasted_iota(jnp.int32, (8, tokens), 0)
    rows = [*targets, weights_ref[0:1, :], weights_ref[1:2, :]]
    table = jnp.zeros((8, tokens), F32)
    for i, values in enumerate(rows):
        table = jnp.where(row == i, values, table)
    cols = jnp.transpose(table)
    cols_ref[...] = cols
    slot_lane = lax.broadcasted_iota(jnp.int32, (tokens, slots), 1)
    for k in range(2):
        target = cols[:, k : k + 1].astype(jnp.int32)
        take_ref[k * tokens : (k + 1) * tokens, :] = (slot_lane == target).astype(F32).astype(BF16)


def later_body(cap, experts, sinks_ref, q_ref, kv_ref, w_ref, routes_ref, weights_ref, out_ref, send_ref, take_ref, cols_ref):
    keys, values = both_places(kv_ref[...].astype(F32))
    inside, _ = window_mask()
    project(attend(q_ref[WINDOW:, :], keys, values, inside, sinks_ref[...]), w_ref, out_ref, WINDOW)
    fill_slots(cap, experts, routes_ref, weights_ref, send_ref, take_ref, cols_ref)


def first_body(sinks_ref, q_ref, kv_ref, before_ref, w_ref, partial_ref, out_ref):
    keys, values = both_places(jnp.concatenate([before_ref[...], kv_ref[:WINDOW, :]], axis=0).astype(F32))
    inside, col = window_mask()
    allowed = inside & ((col >= WINDOW) | (lax.axis_index(SP) > 0))
    project(attend(q_ref[:WINDOW, :], keys, values, allowed, sinks_ref[...]), w_ref, out_ref, 0)


def later_and_slots(sinks, q, kv, w, routes, weights, experts, cap):
    tokens = q.shape[0]
    slots = experts * cap
    return pl.pallas_call(
        functools.partial(later_body, cap, experts),
        out_shape=(
            vmem_out((w.shape[1] // LANES, tokens, LANES)),
            vmem_out((slots, tokens)),
            vmem_out((2 * tokens, slots)),
            pltpu.VMEM((tokens, 8), F32),
        ),
        in_specs=[VMEM_SPEC] * 6,
        out_specs=(VMEM_SPEC,) * 4,
        compiler_params=small_kernel(16),
        cost_estimate=pl.CostEstimate(flops=10**9, bytes_accessed=2**20, transcendentals=2**16),
        name="later_and_slots",
    )(*in_vmem(sinks, q, kv, w, routes, weights))


def attention_first(sinks, q, kv, before, w, partial):
    shares = w.shape[1] // LANES
    return pl.pallas_call(
        first_body,
        out_shape=vmem_out(partial.shape),
        in_specs=[VMEM_SPEC] * 6,
        out_specs=VMEM_SPEC,
        input_output_aliases={5: 0},
        compiler_params=small_kernel(16),
        name="attention_first",
    )(*in_vmem(sinks, q, kv, before, w, partial))


def load_body(*refs):
    sources, (last_ref, kv_ref, sinks_ref, q_ref, w_ref, routes_ref, weights_ref, own_ref) = refs[:8], refs[8:16]
    k_ref, v_ref, sinks_smem, sems = refs[16:]
    k_hbm, v_hbm, q_hbm, w_hbm, sinks_hbm, routes_hbm, weights_hbm, stream_hbm = sources
    first_col = pl.multiple_of(lax.axis_index(TP) * LANES, LANES)
    group = lax.axis_index(TP) * (q_ref.shape[1] // HEAD_DIM) // REP
    heads = pl.ds(pl.multiple_of(group // 2 * LANES, LANES), LANES)
    pairs = (
        (k_hbm.at[:, heads], k_ref),
        (v_hbm.at[:, heads], v_ref),
        (q_hbm, q_ref),
        (w_hbm, w_ref),
        (sinks_hbm, sinks_smem),
        (routes_hbm, routes_ref),
        (weights_hbm, weights_ref),
        (stream_hbm.at[:, pl.ds(first_col, LANES)], own_ref),
    )
    copies = [pltpu.make_async_copy(source, target, sems.at[i]) for i, (source, target) in enumerate(pairs)]
    for copy in copies:
        copy.start()
    low = lax.broadcasted_iota(jnp.int32, kv_ref.shape, 1) < HEAD_DIM

    def head(ref):
        both = ref[...].astype(F32)
        return both, jnp.concatenate([both[:, HEAD_DIM:], both[:, :HEAD_DIM]], axis=1)

    copies[0].wait()
    key, key_swapped = head(k_ref)
    copies[1].wait()
    value, value_swapped = head(v_ref)
    odd = group % 2 == 1
    kv = jnp.where(low, jnp.where(odd, key_swapped, key), jnp.where(odd, value, value_swapped)).astype(BF16)
    kv_ref[...] = kv
    last_ref[...] = kv[kv.shape[0] - WINDOW :]
    copies[4].wait()
    row = lax.broadcasted_iota(jnp.int32, sinks_ref.shape, 0)
    sinks_ref[...] = jnp.where(row == 0, sinks_smem[0], sinks_smem[1])
    for i in (2, 3, 5, 6, 7):
        copies[i].wait()


def loaded(k, v, q, w, sinks, routes, weights, stream_in):
    rows = q.shape[0]
    return pl.pallas_call(
        load_body,
        out_shape=(
            vmem_out((WINDOW, LANES)),
            vmem_out((rows, LANES)),
            pltpu.VMEM((8, LANES), F32),
            vmem_out(q.shape),
            vmem_out(w.shape),
            pltpu.VMEM(routes.shape, jnp.int32),
            pltpu.VMEM(weights.shape, F32),
            vmem_out((rows, LANES)),
        ),
        in_specs=[pl.BlockSpec(memory_space=pltpu.HBM)] * 8,
        out_specs=(VMEM_SPEC,) * 8,
        scratch_shapes=[
            pltpu.VMEM((rows, LANES), BF16),
            pltpu.VMEM((rows, LANES), BF16),
            pltpu.SMEM(sinks.shape, F32),
            pltpu.SemaphoreType.DMA((8,)),
        ],
        compiler_params=small_kernel(16),
        name="load",
    )(*in_hbm(k, v, q, w, sinks, routes, weights, stream_in))


def copies_body(rows_ref, out_ref):
    rows = rows_ref[...]
    for t in range(out_ref.shape[0]):
        out_ref[t] = rows


def copied(rows, count):
    return pl.pallas_call(
        copies_body,
        out_shape=vmem_out((count, *rows.shape)),
        in_specs=[VMEM_SPEC],
        out_specs=VMEM_SPEC,
        compiler_params=small_kernel(16),
        name="copies",
    )(*in_vmem(rows))


def total_body(parts_ref, out_ref):
    rows = parts_ref.shape[1]
    block = 128
    for lo in range(0, rows, block):
        summed = parts_ref[0, lo : lo + block, :].astype(F32)
        for t in range(1, parts_ref.shape[0]):
            summed = summed + parts_ref[t, lo : lo + block, :].astype(F32)
        out_ref[lo : lo + block, :] = summed.astype(BF16)


def total(parts):
    return pl.pallas_call(
        total_body,
        out_shape=vmem_out(parts.shape[1:]),
        in_specs=[VMEM_SPEC],
        out_specs=VMEM_SPEC,
        compiler_params=small_kernel(16),
        name="total",
    )(*in_vmem(parts))


def stream_body(arrived_ref, own_ref, send_ref, stream_ref, rows_ref):
    summed = arrived_ref[0].astype(F32)
    for t in range(1, arrived_ref.shape[0]):
        summed = summed + arrived_ref[t].astype(F32)
    stream = (own_ref[...].astype(F32) + summed).astype(BF16)
    stream_ref[...] = stream
    rows_ref[...] = dot(send_ref[...], stream).astype(BF16)


def stream_and_rows(arrived, own, send):
    return pl.pallas_call(
        stream_body,
        out_shape=(vmem_out(own.shape), vmem_out((send.shape[0], LANES))),
        in_specs=[VMEM_SPEC] * 3,
        out_specs=(VMEM_SPEC, VMEM_SPEC),
        compiler_params=small_kernel(16),
        name="stream",
    )(*in_vmem(arrived, own, send))


def expert_body(block, x_ref, gain_ref, gate_ref, up_ref, down_ref, out_ref):
    shares, rows, _ = x_ref.shape
    flipped = lax.axis_index("core") == 1
    place = [jnp.where(flipped, t % SIDE * SIDE + t // SIDE, t) for t in range(shares)]
    for lo in range(0, rows, block):
        stream = jnp.concatenate([x_ref[place[t], lo : lo + block, :] for t in range(shares)], axis=1).astype(F32)
        scaled = (stream * gain_ref[...]).astype(BF16)
        scale = lax.rsqrt(jnp.mean(stream * stream, axis=-1, keepdims=True) + NORM_EPS)
        gate_act = dot(scaled, gate_ref[0]) * scale
        up_act = dot(scaled, up_ref[0]) * scale
        hidden = (gate_act * jax.nn.sigmoid(gate_act) * up_act).astype(BF16)
        for t in range(0, shares, 2):
            both = dot(hidden, down_ref[0, :, t * LANES : (t + 2) * LANES]).astype(BF16)
            out_ref[place[t], lo : lo + block, :] = both[:, :LANES]
            out_ref[place[t + 1], lo : lo + block, :] = both[:, LANES:]


def expert(x, gain, gate, up, down, block):
    return pl.pallas_call(
        functools.partial(expert_body, block),
        out_shape=vmem_out(x.shape),
        in_specs=[VMEM_SPEC] * 5,
        out_specs=VMEM_SPEC,
        cost_estimate=pl.CostEstimate(flops=6 * x.shape[1] * gate.shape[1] * gate.shape[2], bytes_accessed=2 * x.size * 2, transcendentals=0),
        compiler_params=small_kernel(24),
        name="expert",
    )(*in_vmem(x, gain, gate, up, down))


def combine_body(rows_ref, take_ref, weights_ref, stream_ref, out_ref):
    tokens = stream_ref.shape[0]
    taken = dot(take_ref[...], rows_ref[...])
    moe = taken[:tokens] * weights_ref[:, 2:3] + taken[tokens:] * weights_ref[:, 3:4]
    out_ref[...] = (stream_ref[...].astype(F32) + moe).astype(BF16)


def combine(rows, take, weights, stream):
    return pl.pallas_call(
        combine_body,
        out_shape=vmem_out(stream.shape),
        in_specs=[VMEM_SPEC] * 4,
        out_specs=VMEM_SPEC,
        compiler_params=small_kernel(16),
        name="combine",
    )(*in_vmem(rows, take, weights, stream))


def lines(core, dim):
    at = [[core * SIDE * SIDE + y * SIDE + x for x in range(SIDE)] for y in range(SIDE)]
    return at if dim == 1 else [list(line) for line in zip(*at)]


LINES = lines(0, 1) + lines(1, 0)
CROSSING = lines(0, 0) + lines(1, 1)


def along(parts, groups):
    return lax.all_to_all(parts, PLANES, split_axis=0, concat_axis=0, axis_index_groups=groups, tiled=True)


def per_device(
    query_rows,
    key_rows,
    value_rows,
    sink_logits,
    out_weight,
    stream_in,
    norm_gain,
    routes,
    route_weights,
    gate_weight,
    up_weight,
    down_weight,
):
    tokens = query_rows.shape[0]
    tp_size = lax.axis_size(TP)
    experts = lax.axis_size(SP)
    cap = 3 * tokens * routes.shape[1] // (2 * experts)
    last, kv, sinks, queries, out_share, choices, weights, own = loaded(
        key_rows, value_rows, query_rows, out_weight, sink_logits, routes.T, route_weights.T, stream_in
    )
    before = lax.ppermute(last, SP, [(i, i + 1) for i in range(experts - 1)])
    later, send, take, cols = later_and_slots(sinks, queries, kv, out_share, choices, weights, experts, cap)
    partial = attention_first(sinks, queries, kv, before, out_share, later)
    arrived = lax.all_to_all(partial, TP, split_axis=0, concat_axis=0, tiled=True)
    stream, rows = stream_and_rows(arrived, own, send)
    rows = lax.all_to_all(rows.reshape(experts, cap, LANES), SP, split_axis=0, concat_axis=0, tiled=True)
    slots = experts * cap
    gain = norm_gain.reshape(1, -1)
    features = rows.reshape(slots, LANES)
    for groups in (LINES, CROSSING):
        features = along(copied(features, SIDE), groups).reshape(-1, LANES)
    parts = expert(features.reshape(tp_size, slots, LANES), gain, gate_weight, up_weight, down_weight, slots)
    for groups in (CROSSING, LINES):
        parts = total(along(parts.reshape(SIDE, -1, LANES), groups))
    summed = parts
    returned = lax.all_to_all(summed.reshape(experts, cap, LANES), SP, split_axis=0, concat_axis=0, tiled=True)
    out = combine(returned.reshape(slots, LANES), take, cols, stream)
    return lax.all_to_all(out, TP, split_axis=0, concat_axis=1, tiled=True)


def solution(mesh):
    finer = Mesh(mesh.devices.reshape(-1, 2, SIDE, SIDE), (*SP, *TP))
    placed = (
        P(SP, TP),
        P(SP, None),
        P(SP, None),
        P(TP),
        P(TP, None),
        P(SP, None),
        P(),
        P(SP, None),
        P(SP, None),
        P(SP, None, TP),
        P(SP, None, TP),
        P(SP, TP, None),
    )
    return jax.shard_map(
        per_device, mesh=finer, in_specs=placed, out_specs=P((*SP, *TP), None), check_vma=False
    )
```

```python
import functools

import jax
import jax.numpy as jnp
from jax import lax
from jax.experimental import pallas as pl
from jax.experimental.pallas import tpu as pltpu
from jax.sharding import Mesh
from jax.sharding import PartitionSpec as P

HEAD_DIM = 64
REP = 8
WINDOW = 128
LANES = 128
TP = ("tp_0", "tp_1")
SP = ("z", "core")
PLANES = ("core", "tp_0", "tp_1")
SIDE = 4
NORM_EPS = 1e-06
BF16 = jnp.bfloat16
F32 = jnp.float32
VMEM_SPEC = pl.BlockSpec(memory_space=pltpu.VMEM)


def in_vmem(*arrays):
    return [pltpu.with_memory_space_constraint(a, pltpu.VMEM) for a in arrays]


def in_hbm(*arrays):
    return [pltpu.with_memory_space_constraint(a, pltpu.HBM) for a in arrays]


def small_kernel(mib):
    return pltpu.CompilerParams(vmem_limit_bytes=mib * 2**20)


def vmem_out(shape):
    return pltpu.VMEM(shape, BF16)


def dot(a, b, contract=(1, 0)):
    return lax.dot_general(a, b, (((contract[0],), (contract[1],)), ((), ())), preferred_element_type=F32)


def both_places(block):
    swapped = jnp.concatenate([block[:, HEAD_DIM:], block[:, :HEAD_DIM]], axis=1)
    low = lax.broadcasted_iota(jnp.int32, block.shape, 1) < HEAD_DIM
    zero = jnp.zeros_like(block)
    keys = (jnp.where(low, block, zero), jnp.where(low, zero, swapped))
    values = (jnp.where(low, swapped, zero), jnp.where(low, zero, block))
    return [k.astype(BF16) for k in keys], [v.astype(BF16) for v in values]


def attend(q, keys, values, allowed, sinks):
    total = None
    for h in range(2):
        scores = dot(q, keys[h], (1, 1)) * HEAD_DIM**-0.5
        scores = jnp.where(allowed, scores, -1e30)
        sink = sinks[h : h + 1, :1]
        peak = jnp.maximum(jnp.max(scores, axis=-1, keepdims=True), sink)
        terms = jnp.exp(scores - peak)
        total_terms = jnp.sum(terms, axis=-1, keepdims=True) + jnp.exp(sink - peak)
        probs = (terms / total_terms).astype(BF16)
        part = dot(probs, values[h])
        total = part if total is None else total + part
    return total.astype(BF16)


def project(attended, w_ref, out_ref, row0):
    for t in range(0, out_ref.shape[0], 2):
        both = dot(attended, w_ref[:, t * LANES : (t + 2) * LANES]).astype(BF16)
        out_ref[t, row0 : row0 + WINDOW, :] = both[:, :LANES]
        out_ref[t + 1, row0 : row0 + WINDOW, :] = both[:, LANES:]


def window_mask():
    row = lax.broadcasted_iota(jnp.int32, (WINDOW, 2 * WINDOW), 0)
    col = lax.broadcasted_iota(jnp.int32, (WINDOW, 2 * WINDOW), 1)
    return (col > row) & (col <= row + WINDOW), col


def fill_slots(cap, experts, routes_ref, weights_ref, send_ref, take_ref, cols_ref):
    tokens = routes_ref.shape[1]
    slots = send_ref.shape[0]
    expert_row = lax.broadcasted_iota(jnp.int32, (experts, tokens), 0)
    picks = [routes_ref[k : k + 1, :] for k in range(2)]
    hot = [(pick == expert_row).astype(F32) for pick in picks]
    r = lax.broadcasted_iota(jnp.int32, (tokens, tokens), 0)
    c = lax.broadcasted_iota(jnp.int32, (tokens, tokens), 1)
    ahead = dot((hot[0] + hot[1]).astype(BF16), (r < c).astype(BF16))
    targets = [picks[k].astype(F32) * cap + jnp.sum(ahead * hot[k], axis=0, keepdims=True) for k in range(2)]
    slot_row = lax.broadcasted_iota(jnp.int32, (slots, tokens), 0)
    here = [slot_row == target.astype(jnp.int32) for target in targets]
    send_ref[...] = (here[0] | here[1]).astype(F32).astype(BF16)
    row = lax.broadcasted_iota(jnp.int32, (8, tokens), 0)
    rows = [*targets, weights_ref[0:1, :], weights_ref[1:2, :]]
    table = jnp.zeros((8, tokens), F32)
    for i, values in enumerate(rows):
        table = jnp.where(row == i, values, table)
    cols = jnp.transpose(table)
    cols_ref[...] = cols
    slot_lane = lax.broadcasted_iota(jnp.int32, (tokens, slots), 1)
    for k in range(2):
        target = cols[:, k : k + 1].astype(jnp.int32)
        take_ref[k * tokens : (k + 1) * tokens, :] = (slot_lane == target).astype(F32).astype(BF16)


def later_body(cap, experts, sinks_ref, q_ref, kv_ref, w_ref, routes_ref, weights_ref, out_ref, send_ref, take_ref, cols_ref):
    keys, values = both_places(kv_ref[...].astype(F32))
    inside, _ = window_mask()
    project(attend(q_ref[WINDOW:, :], keys, values, inside, sinks_ref[...]), w_ref, out_ref, WINDOW)
    fill_slots(cap, experts, routes_ref, weights_ref, send_ref, take_ref, cols_ref)


def first_body(sinks_ref, q_ref, kv_ref, before_ref, w_ref, partial_ref, out_ref):
    keys, values = both_places(jnp.concatenate([before_ref[...], kv_ref[:WINDOW, :]], axis=0).astype(F32))
    inside, col = window_mask()
    allowed = inside & ((col >= WINDOW) | (lax.axis_index(SP) > 0))
    project(attend(q_ref[:WINDOW, :], keys, values, allowed, sinks_ref[...]), w_ref, out_ref, 0)


def later_and_slots(sinks, q, kv, w, routes, weights, experts, cap):
    tokens = q.shape[0]
    slots = experts * cap
    return pl.pallas_call(
        functools.partial(later_body, cap, experts),
        out_shape=(
            vmem_out((w.shape[1] // LANES, tokens, LANES)),
            vmem_out((slots, tokens)),
            vmem_out((2 * tokens, slots)),
            pltpu.VMEM((tokens, 8), F32),
        ),
        in_specs=[VMEM_SPEC] * 6,
        out_specs=(VMEM_SPEC,) * 4,
        compiler_params=small_kernel(16),
        cost_estimate=pl.CostEstimate(flops=10**9, bytes_accessed=2**20, transcendentals=2**16),
        name="later_and_slots",
    )(*in_vmem(sinks, q, kv, w, routes, weights))


def attention_first(sinks, q, kv, before, w, partial):
    shares = w.shape[1] // LANES
    return pl.pallas_call(
        first_body,
        out_shape=vmem_out(partial.shape),
        in_specs=[VMEM_SPEC] * 6,
        out_specs=VMEM_SPEC,
        input_output_aliases={5: 0},
        compiler_params=small_kernel(16),
        name="attention_first",
    )(*in_vmem(sinks, q, kv, before, w, partial))


def load_body(*refs):
    sources, (last_ref, kv_ref, sinks_ref, q_ref, w_ref, routes_ref, weights_ref, own_ref) = refs[:8], refs[8:16]
    k_ref, v_ref, sinks_smem, sems = refs[16:]
    k_hbm, v_hbm, q_hbm, w_hbm, sinks_hbm, routes_hbm, weights_hbm, stream_hbm = sources
    first_col = pl.multiple_of(lax.axis_index(TP) * LANES, LANES)
    group = lax.axis_index(TP) * (q_ref.shape[1] // HEAD_DIM) // REP
    heads = pl.ds(pl.multiple_of(group // 2 * LANES, LANES), LANES)
    pairs = (
        (k_hbm.at[:, heads], k_ref),
        (v_hbm.at[:, heads], v_ref),
        (q_hbm, q_ref),
        (w_hbm, w_ref),
        (sinks_hbm, sinks_smem),
        (routes_hbm, routes_ref),
        (weights_hbm, weights_ref),
        (stream_hbm.at[:, pl.ds(first_col, LANES)], own_ref),
    )
    copies = [pltpu.make_async_copy(source, target, sems.at[i]) for i, (source, target) in enumerate(pairs)]
    for copy in copies:
        copy.start()
    low = lax.broadcasted_iota(jnp.int32, kv_ref.shape, 1) < HEAD_DIM

    def head(ref):
        both = ref[...].astype(F32)
        return both, jnp.concatenate([both[:, HEAD_DIM:], both[:, :HEAD_DIM]], axis=1)

    copies[0].wait()
    key, key_swapped = head(k_ref)
    copies[1].wait()
    value, value_swapped = head(v_ref)
    odd = group % 2 == 1
    kv = jnp.where(low, jnp.where(odd, key_swapped, key), jnp.where(odd, value, value_swapped)).astype(BF16)
    kv_ref[...] = kv
    last_ref[...] = kv[kv.shape[0] - WINDOW :]
    copies[4].wait()
    row = lax.broadcasted_iota(jnp.int32, sinks_ref.shape, 0)
    sinks_ref[...] = jnp.where(row == 0, sinks_smem[0], sinks_smem[1])
    for i in (2, 3, 5, 6, 7):
        copies[i].wait()


def loaded(k, v, q, w, sinks, routes, weights, stream_in):
    rows = q.shape[0]
    return pl.pallas_call(
        load_body,
        out_shape=(
            vmem_out((WINDOW, LANES)),
            vmem_out((rows, LANES)),
            pltpu.VMEM((8, LANES), F32),
            vmem_out(q.shape),
            vmem_out(w.shape),
            pltpu.VMEM(routes.shape, jnp.int32),
            pltpu.VMEM(weights.shape, F32),
            vmem_out((rows, LANES)),
        ),
        in_specs=[pl.BlockSpec(memory_space=pltpu.HBM)] * 8,
        out_specs=(VMEM_SPEC,) * 8,
        scratch_shapes=[
            pltpu.VMEM((rows, LANES), BF16),
            pltpu.VMEM((rows, LANES), BF16),
            pltpu.SMEM(sinks.shape, F32),
            pltpu.SemaphoreType.DMA((8,)),
        ],
        compiler_params=small_kernel(16),
        name="load",
    )(*in_hbm(k, v, q, w, sinks, routes, weights, stream_in))


def copies_body(rows_ref, out_ref):
    rows = rows_ref[...]
    for t in range(out_ref.shape[0]):
        out_ref[t] = rows


def copied(rows, count):
    return pl.pallas_call(
        copies_body,
        out_shape=vmem_out((count, *rows.shape)),
        in_specs=[VMEM_SPEC],
        out_specs=VMEM_SPEC,
        compiler_params=small_kernel(16),
        name="copies",
    )(*in_vmem(rows))


def total_body(parts_ref, out_ref):
    rows = parts_ref.shape[1]
    block = 256
    for lo in range(0, rows, block):
        summed = parts_ref[0, lo : lo + block, :].astype(F32)
        for t in range(1, parts_ref.shape[0]):
            summed = summed + parts_ref[t, lo : lo + block, :].astype(F32)
        out_ref[lo : lo + block, :] = summed.astype(BF16)


def total(parts):
    return pl.pallas_call(
        total_body,
        out_shape=vmem_out(parts.shape[1:]),
        in_specs=[VMEM_SPEC],
        out_specs=VMEM_SPEC,
        compiler_params=small_kernel(16),
        name="total",
    )(*in_vmem(parts))


def stream_body(arrived_ref, own_ref, send_ref, stream_ref, rows_ref):
    summed = arrived_ref[0].astype(F32)
    for t in range(1, arrived_ref.shape[0]):
        summed = summed + arrived_ref[t].astype(F32)
    stream = (own_ref[...].astype(F32) + summed).astype(BF16)
    stream_ref[...] = stream
    rows_ref[...] = dot(send_ref[...], stream).astype(BF16)


def stream_and_rows(arrived, own, send):
    return pl.pallas_call(
        stream_body,
        out_shape=(vmem_out(own.shape), vmem_out((send.shape[0], LANES))),
        in_specs=[VMEM_SPEC] * 3,
        out_specs=(VMEM_SPEC, VMEM_SPEC),
        compiler_params=small_kernel(16),
        name="stream",
    )(*in_vmem(arrived, own, send))


def expert_body(block, x_ref, gain_ref, gate_ref, up_ref, down_ref, out_ref):
    shares, rows, _ = x_ref.shape
    flipped = lax.axis_index("core") == 1
    place = [jnp.where(flipped, t % SIDE * SIDE + t // SIDE, t) for t in range(shares)]
    for lo in range(0, rows, block):
        stream = jnp.concatenate([x_ref[place[t], lo : lo + block, :] for t in range(shares)], axis=1).astype(F32)
        scaled = (stream * gain_ref[...]).astype(BF16)
        scale = lax.rsqrt(jnp.mean(stream * stream, axis=-1, keepdims=True) + NORM_EPS)
        gate_act = dot(scaled, gate_ref[0]) * scale
        up_act = dot(scaled, up_ref[0]) * scale
        hidden = (gate_act * jax.nn.sigmoid(gate_act) * up_act).astype(BF16)
        for t in range(0, shares, 2):
            both = dot(hidden, down_ref[0, :, t * LANES : (t + 2) * LANES]).astype(BF16)
            out_ref[place[t], lo : lo + block, :] = both[:, :LANES]
            out_ref[place[t + 1], lo : lo + block, :] = both[:, LANES:]


def expert(x, gain, gate, up, down, block):
    return pl.pallas_call(
        functools.partial(expert_body, block),
        out_shape=vmem_out(x.shape),
        in_specs=[VMEM_SPEC] * 5,
        out_specs=VMEM_SPEC,
        cost_estimate=pl.CostEstimate(flops=6 * x.shape[1] * gate.shape[1] * gate.shape[2], bytes_accessed=2 * x.size * 2, transcendentals=0),
        compiler_params=small_kernel(24),
        name="expert",
    )(*in_vmem(x, gain, gate, up, down))


def combine_body(rows_ref, take_ref, weights_ref, stream_ref, out_ref):
    tokens = stream_ref.shape[0]
    taken = dot(take_ref[...], rows_ref[...])
    moe = taken[:tokens] * weights_ref[:, 2:3] + taken[tokens:] * weights_ref[:, 3:4]
    out_ref[...] = (stream_ref[...].astype(F32) + moe).astype(BF16)


def combine(rows, take, weights, stream):
    return pl.pallas_call(
        combine_body,
        out_shape=vmem_out(stream.shape),
        in_specs=[VMEM_SPEC] * 4,
        out_specs=VMEM_SPEC,
        compiler_params=small_kernel(16),
        name="combine",
    )(*in_vmem(rows, take, weights, stream))


def lines(core, dim):
    at = [[core * SIDE * SIDE + y * SIDE + x for x in range(SIDE)] for y in range(SIDE)]
    return at if dim == 1 else [list(line) for line in zip(*at)]


LINES = lines(0, 1) + lines(1, 0)
CROSSING = lines(0, 0) + lines(1, 1)


def along(parts, groups):
    return lax.all_to_all(parts, PLANES, split_axis=0, concat_axis=0, axis_index_groups=groups, tiled=True)


def per_device(
    query_rows,
    key_rows,
    value_rows,
    sink_logits,
    out_weight,
    stream_in,
    norm_gain,
    routes,
    route_weights,
    gate_weight,
    up_weight,
    down_weight,
):
    tokens = query_rows.shape[0]
    tp_size = lax.axis_size(TP)
    experts = lax.axis_size(SP)
    cap = 3 * tokens * routes.shape[1] // (2 * experts)
    last, kv, sinks, queries, out_share, choices, weights, own = loaded(
        key_rows, value_rows, query_rows, out_weight, sink_logits, routes.T, route_weights.T, stream_in
    )
    before = lax.ppermute(last, SP, [(i, i + 1) for i in range(experts - 1)])
    later, send, take, cols = later_and_slots(sinks, queries, kv, out_share, choices, weights, experts, cap)
    partial = attention_first(sinks, queries, kv, before, out_share, later)
    arrived = lax.all_to_all(partial, TP, split_axis=0, concat_axis=0, tiled=True)
    stream, rows = stream_and_rows(arrived, own, send)
    rows = lax.all_to_all(rows.reshape(experts, cap, LANES), SP, split_axis=0, concat_axis=0, tiled=True)
    slots = experts * cap
    gain = norm_gain.reshape(1, -1)
    features = rows.reshape(slots, LANES)
    for groups in (LINES, CROSSING):
        features = along(copied(features, SIDE), groups).reshape(-1, LANES)
    parts = expert(features.reshape(tp_size, slots, LANES), gain, gate_weight, up_weight, down_weight, slots)
    for groups in (CROSSING, LINES):
        parts = total(along(parts.reshape(SIDE, -1, LANES), groups))
    summed = parts
    returned = lax.all_to_all(summed.reshape(experts, cap, LANES), SP, split_axis=0, concat_axis=0, tiled=True)
    out = combine(returned.reshape(slots, LANES), take, cols, stream)
    return lax.all_to_all(out, TP, split_axis=0, concat_axis=1, tiled=True)


def solution(mesh):
    finer = Mesh(mesh.devices.reshape(-1, 2, SIDE, SIDE), (*SP, *TP))
    placed = (
        P(SP, TP),
        P(SP, None),
        P(SP, None),
        P(TP),
        P(TP, None),
        P(SP, None),
        P(),
        P(SP, None),
        P(SP, None),
        P(SP, None, TP),
        P(SP, None, TP),
        P(SP, TP, None),
    )
    return jax.shard_map(
        per_device, mesh=finer, in_specs=placed, out_specs=P((*SP, *TP), None), check_vma=False
    )
```
